512 devices in a mesh: sp: 64 (over z, y), tp: 8 (over x, core).
Axes of the slice: x: 4, y: 4, z: 16, core: 2. Of those that a mesh axis runs over, the one named last changes fastest.
Arguments:
- tokens: bfloat16 [8192, 2048], P('sp'), may hold values from -6 to 6
- input_norm_scale: float32 [2048], replicated, may hold values from 0.1 to 1.9
- input_norm_bias: float32 [2048], replicated, may hold values from -2 to 2
- query_projection: bfloat16 [2048, 1024], P('sp', 'tp'), may hold values from -0.125 to 0.125
- key_projection: bfloat16 [2048, 1024], P('sp', 'tp'), may hold values from -0.125 to 0.125
- value_projection: bfloat16 [2048, 1024], P('sp', 'tp'), may hold values from -0.125 to 0.125
- pooling_input_projection: bfloat16 [2048, 1024], P('sp', 'tp'), may hold values from -0.125 to 0.125
- decay_input_weight: bfloat16 [2048, 128], P('sp'), may hold values from -0.125 to 0.125
- rate_input_weight: bfloat16 [2048, 128], P('sp'), may hold values from -0.125 to 0.125
- gate_input_weight: bfloat16 [2048, 256], P('sp'), may hold values from -0.125 to 0.125
- decay_output_weight: bfloat16 [128, 1024], P(None, 'tp'), may hold values from -0.5 to 0.5
- rate_output_weight: bfloat16 [128, 1024], P(None, 'tp'), may hold values from -0.5 to 0.5
- gate_output_weight: bfloat16 [256, 1024], P(None, 'tp'), may hold values from -0.375 to 0.375
- decay_bias_base: float32 [1024], P('tp'), may hold values from -13 to -2.5
- learning_rate_base: float32 [1024], P('tp'), may hold values from -4 to 4
- key_prenorm_scale: float32 [1024], P('tp'), may hold values from 0.1 to 1.9
- key_learning_scale: float32 [1024], P('tp'), may hold values from 0.1 to 1.9
- self_term_weight: float32 [1024], P('tp'), may hold values from -3 to 3
- head_norm_scale: float32 [1024], P('tp'), may hold values from 0.1 to 1.9
- head_norm_bias: float32 [1024], P('tp'), may hold values from -3 to 3
- rate_extra_log: float32 [8192, 1024], P('sp', 'tp'), may hold values from -0.7 to 0.7
- decay_extra_log: float32 [8192, 1024], P('sp', 'tp'), may hold values from -0.7 to 0
- starting_head_state: float32 [16, 64, 64], P('tp'), may hold values from -12 to 12
- pooling_group_matrix: bfloat16 [8, 128, 128], P('tp'), may hold values from -0.5 to 0.5
- pooling_output_scale: float32 [1024], P('tp'), may hold values from 0.1 to 1.9
- output_attention_rows: bfloat16 [1024, 2048], P('tp', 'sp'), may hold values from -0.125 to 0.125
- output_pooling_rows: bfloat16 [1024, 2048], P('tp', 'sp'), may hold values from -0.125 to 0.125
Outputs:
- mixed: bfloat16 [8192, 2048], P(('sp', 'tp'))
The draws below stay inside these ranges and needn't reach their ends.
All inputs are finite; a program needn't handle non-finite values.
Results may differ from the reference program's by a relative error of at most 0.019.
Values may be sent and summed in bfloat16 or wider, within the bound.
No kernel may reach another device: no remote copies, remote signals or barrier semaphores. Data moves between devices by JAX's collectives and lax.ppermute only.
A program may use at most 64 MiB of HBM per device.

```python
import jax
import jax.numpy as jnp
from jax import lax

D = 2048
HEAD_CHANNELS = 64
RWKV_HEADS = 16
POOL_GROUPS = 8
POOL_GROUP = 128
DECAY_RANK = 128
RATE_RANK = 128
GATE_RANK = 256
TOK_DEV = 128
MIXER_CHANNELS = 1024
POOL_WIDTH = 1024
SEQUENCE_LENGTH = 8192
N_TP = 8


def draw_decay_bias_base(key, part):
    first, second, third = jax.random.split(jax.random.fold_in(key, 11), 3)
    share = 0.5
    slow_heads = jax.random.uniform(first, (RWKV_HEADS,), jnp.float32) < share
    slow_mask = jnp.repeat(slow_heads, HEAD_CHANNELS)
    slow_value = jnp.log(0.5 / SEQUENCE_LENGTH) + jax.random.uniform(second, (MIXER_CHANNELS,), jnp.float32, -1.5, 0.5)
    fast_value = jax.random.uniform(third, (MIXER_CHANNELS,), jnp.float32, -3.5, -2.5)
    return jnp.where(slow_mask, slow_value, fast_value).astype(jnp.float32)


def draw_rate_extra_log(key, part):
    blocks = SEQUENCE_LENGTH // TOK_DEV
    level = jax.random.uniform(jax.random.fold_in(key, 22), (blocks, RWKV_HEADS), jnp.float32, -0.7, 0.7)
    level = jnp.repeat(level, TOK_DEV, axis=0)
    return jnp.repeat(level, HEAD_CHANNELS, axis=1).astype(jnp.float32)


def draw_decay_extra_log(key, part):
    first, second = jax.random.split(jax.random.fold_in(key, 31), 2)
    expected_output = 8.0
    rate_probability = jax.random.uniform(first, (SEQUENCE_LENGTH, RWKV_HEADS), jnp.float32)
    stack_depth = jax.random.uniform(second, (SEQUENCE_LENGTH, RWKV_HEADS), jnp.float32, 0.2, 0.5)
    decay_offset = jnp.where(rate_probability < expected_output / SEQUENCE_LENGTH, jnp.log1p(-stack_depth), 0.0)
    return jnp.repeat(decay_offset, HEAD_CHANNELS, axis=1).astype(jnp.float32)


def levels(stream_key, extent, shards, smallest, largest):
    factor_of = 1.0
    for axis_at, parts in shards:
        heights = jax.random.uniform(jax.random.fold_in(jax.random.fold_in(stream_key, 6), axis_at), (parts,), jnp.float32, smallest / len(shards), largest / len(shards))
        factor_of = factor_of * jnp.repeat(jnp.exp(heights), extent[axis_at] // parts).reshape((-1,) + (1,) * (len(extent) - 1 - axis_at))
    return factor_of


def centred(own_key, shape, scale, reach, shards=(), held_as=jnp.bfloat16):
    values = jax.random.normal(own_key, shape, jnp.float32) * scale
    if len(shards) > 0:
        values = levels(own_key, shape, shards, -0.22, 0.18) * values
    return jnp.clip(values, min=-reach, max=reach).astype(held_as)


def setup_inputs(seed: int = 0) -> dict:
    seeds = jax.random.split(jax.random.key(seed), 28)
    tokens = centred(seeds[0], (SEQUENCE_LENGTH, D), 1.0, 6.0, ((0, 64),))
    input_norm_scale = jnp.clip(1.0 + 0.18 * jax.random.normal(seeds[1], (D,), jnp.float32), 0.1, 1.9)
    input_norm_bias = centred(seeds[2], (D,), 0.3, 2.0, (), jnp.float32)
    query_projection = centred(seeds[3], (D, MIXER_CHANNELS), D ** -0.5, 0.125, ((0, 64), (1, 8)))
    key_projection = centred(seeds[4], (D, MIXER_CHANNELS), D ** -0.5, 0.125, ((0, 64), (1, 8)))
    value_projection = centred(seeds[5], (D, MIXER_CHANNELS), D ** -0.5, 0.125, ((0, 64), (1, 8)))
    pooling_input_projection = centred(seeds[6], (D, POOL_WIDTH), D ** -0.5, 0.125, ((0, 64), (1, 8)))
    decay_input_weight = centred(seeds[7], (D, DECAY_RANK), D ** -0.5, 0.125, ((0, 64),))
    rate_input_weight = centred(seeds[8], (D, RATE_RANK), D ** -0.5, 0.125, ((0, 64),))
    gate_input_weight = centred(seeds[9], (D, GATE_RANK), D ** -0.5, 0.125, ((0, 64),))
    decay_output_weight = centred(seeds[10], (DECAY_RANK, MIXER_CHANNELS), DECAY_RANK ** -0.5, 0.5, ((1, 8),))
    rate_output_weight = centred(seeds[11], (RATE_RANK, MIXER_CHANNELS), RATE_RANK ** -0.5, 0.5, ((1, 8),))
    gate_output_weight = centred(seeds[12], (GATE_RANK, MIXER_CHANNELS), GATE_RANK ** -0.5, 0.375, ((1, 8),))
    decay_bias_base = draw_decay_bias_base(jax.random.fold_in(seeds[27], 71), 0)
    learning_rate_base = centred(seeds[14], (MIXER_CHANNELS,), 1.0, 4.0, ((0, 8),), jnp.float32)
    key_prenorm_scale = jnp.clip(1.0 + 0.18 * jax.random.normal(seeds[15], (MIXER_CHANNELS,), jnp.float32), 0.1, 1.9)
    key_learning_scale = jnp.clip(1.0 + 0.18 * jax.random.normal(seeds[16], (MIXER_CHANNELS,), jnp.float32), 0.1, 1.9)
    self_term_weight = centred(seeds[17], (MIXER_CHANNELS,), 0.5, 3.0, ((0, 8),), jnp.float32)
    head_norm_scale = jnp.clip(1.0 + 0.18 * jax.random.normal(seeds[18], (MIXER_CHANNELS,), jnp.float32), 0.1, 1.9)
    head_norm_bias = centred(seeds[19], (MIXER_CHANNELS,), 0.5, 3.0, ((0, 8),), jnp.float32)
    rate_extra_log = draw_rate_extra_log(jax.random.fold_in(seeds[27], 71), 0)
    decay_extra_log = draw_decay_extra_log(jax.random.fold_in(seeds[27], 71), 0)
    starting_head_state = centred(seeds[22], (RWKV_HEADS, HEAD_CHANNELS, HEAD_CHANNELS), 2.0, 12.0, ((0, 8),), jnp.float32)
    pooling_group_matrix = centred(seeds[23], (POOL_GROUPS, POOL_GROUP, POOL_GROUP), POOL_GROUP ** -0.5, 0.5, ((0, 8),))
    pooling_output_scale = jnp.clip(1.0 + 0.18 * jax.random.normal(seeds[24], (POOL_WIDTH,), jnp.float32), 0.1, 1.9)
    output_attention_rows = centred(seeds[25], (MIXER_CHANNELS, D), D ** -0.5, 0.125, ((0, 8), (1, 64)))
    output_pooling_rows = centred(seeds[26], (POOL_WIDTH, D), D ** -0.5, 0.125, ((0, 8), (1, 64)))
    return dict(tokens=tokens, input_norm_scale=input_norm_scale, input_norm_bias=input_norm_bias, query_projection=query_projection, key_projection=key_projection, value_projection=value_projection, pooling_input_projection=pooling_input_projection, decay_input_weight=decay_input_weight, rate_input_weight=rate_input_weight, gate_input_weight=gate_input_weight, decay_output_weight=decay_output_weight, rate_output_weight=rate_output_weight, gate_output_weight=gate_output_weight, decay_bias_base=decay_bias_base, learning_rate_base=learning_rate_base, key_prenorm_scale=key_prenorm_scale, key_learning_scale=key_learning_scale, self_term_weight=self_term_weight, head_norm_scale=head_norm_scale, head_norm_bias=head_norm_bias, rate_extra_log=rate_extra_log, decay_extra_log=decay_extra_log, starting_head_state=starting_head_state, pooling_group_matrix=pooling_group_matrix, pooling_output_scale=pooling_output_scale, output_attention_rows=output_attention_rows, output_pooling_rows=output_pooling_rows)


pool_windows = (2, 4, 8, 16)
pool_reach = 16

def layer_normed(values, gain, bias):
    wide = values.astype(jnp.float32)
    center = lax.optimization_barrier(jnp.mean(wide, axis=-1, keepdims=True))
    spread = lax.optimization_barrier(jnp.mean(jnp.square(wide - center), axis=-1, keepdims=True))
    return ((wide - center) * lax.rsqrt(spread + 1e-05) * gain + bias).astype(jnp.bfloat16)

def delta_step(state, inputs):
    recv, decay_t, key_t, value_t, alpha_t, beta_t = inputs
    along = jnp.einsum('hvk,hk->hv', state, alpha_t, precision=lax.Precision.HIGHEST)
    state = state * decay_t[:, None, :] + along[:, :, None] * beta_t[:, None, :] + value_t[:, :, None] * key_t[:, None, :]
    reading = jnp.einsum('hvk,hk->hv', state, recv, precision=lax.Precision.HIGHEST)
    return (state, reading)

def window_width(scale_index):
    result = jnp.zeros(scale_index.shape, jnp.float32)
    for level, width in enumerate(pool_windows):
        result = jnp.where(scale_index == level, jnp.float32(width), result)
    return result

def window_sums(extended, scale_index, row_total):
    running = jnp.zeros((row_total, extended.shape[1]), jnp.float32)
    chosen = jnp.zeros((row_total, extended.shape[1]), jnp.float32)
    for offset in range(pool_reach):
        running = running + extended[pool_reach - offset:pool_reach - offset + row_total]
        for level, width in enumerate(pool_windows):
            if offset + 1 == width:
                chosen = jnp.where(scale_index[None, :] == level, running, chosen)
    return chosen

def reference(tokens, input_norm_scale, input_norm_bias, query_projection, key_projection, value_projection, pooling_input_projection, decay_input_weight, rate_input_weight, gate_input_weight, decay_output_weight, rate_output_weight, gate_output_weight, decay_bias_base, learning_rate_base, key_prenorm_scale, key_learning_scale, self_term_weight, head_norm_scale, head_norm_bias, rate_extra_log, decay_extra_log, starting_head_state, pooling_group_matrix, pooling_output_scale, output_attention_rows, output_pooling_rows):
    f32 = jnp.float32
    bf16 = jnp.bfloat16
    normed = layer_normed(tokens, input_norm_scale, input_norm_bias)

    def project(weight):
        return jnp.dot(normed, weight, preferred_element_type=f32).astype(bf16)
    recept, keys, values, pool_in = (project(query_projection), project(key_projection), project(value_projection), project(pooling_input_projection))
    decay_low, rate_low, gate_low = (project(decay_input_weight), project(rate_input_weight), project(gate_input_weight))
    decay_tanh = jnp.tanh(decay_low.astype(f32)).astype(bf16)
    gate_sig = jax.nn.sigmoid(gate_low.astype(f32)).astype(bf16)
    rate_logarithm = -jax.nn.softplus(-(decay_bias_base + jnp.dot(decay_tanh, decay_output_weight, preferred_element_type=f32))) - 0.5 + rate_extra_log
    decay_factor = jnp.exp(-jnp.exp(rate_logarithm) + decay_extra_log)
    rate = jax.nn.sigmoid(learning_rate_base + jnp.dot(rate_low, rate_output_weight, preferred_element_type=f32))
    gate = jnp.dot(gate_sig, gate_output_weight, preferred_element_type=f32)
    row_total = tokens.shape[0]

    def head_number(array):
        return array.astype(f32).reshape(row_total, RWKV_HEADS, HEAD_CHANNELS)

    def channel_heads(vector):
        return vector.astype(f32).reshape(RWKV_HEADS, HEAD_CHANNELS)
    key_wide = keys.astype(f32)
    unit = head_number(key_wide * key_prenorm_scale)
    unit = unit * lax.rsqrt(lax.optimization_barrier(jnp.sum(unit * unit, axis=-1, keepdims=True)) + 1e-06)
    effective_key = head_number(key_wide * (1.0 + (rate - 1.0) * key_learning_scale))
    query_per_head, value_per_head = (head_number(recept), head_number(values))
    _, reading = lax.scan(delta_step, starting_head_state.astype(f32), (query_per_head, head_number(decay_factor), effective_key, value_per_head, -unit, unit * head_number(rate)))
    center = lax.optimization_barrier(jnp.mean(reading, axis=-1, keepdims=True))
    spread = lax.optimization_barrier(jnp.mean(jnp.square(reading - center), axis=-1, keepdims=True))
    split_by_head = (reading - center) * lax.rsqrt(spread + 1e-05 * HEAD_CHANNELS) * channel_heads(head_norm_scale) + channel_heads(head_norm_bias)
    split_by_head = split_by_head + lax.optimization_barrier(jnp.sum(query_per_head * effective_key * channel_heads(self_term_weight), axis=-1, keepdims=True)) * value_per_head
    attn_out = (split_by_head.reshape(row_total, MIXER_CHANNELS) * gate).astype(bf16)
    pool_wide = pool_in.astype(f32)
    extended = jnp.concatenate([jnp.zeros((pool_reach, POOL_WIDTH), f32), pool_wide], axis=0)
    scale_index = jnp.arange(POOL_WIDTH, dtype=jnp.int32) // POOL_GROUP // (POOL_GROUPS // 4)
    chosen = window_sums(extended, scale_index, row_total)
    position = jnp.arange(row_total, dtype=jnp.int32).astype(f32)
    counted = jnp.minimum(position[:, None] + 1.0, window_width(scale_index)[None, :])
    pooled = (chosen / counted - pool_wide).astype(bf16)
    grouped = jnp.einsum('tgc,gcd->tgd', pooled.reshape(row_total, POOL_GROUPS, POOL_GROUP).astype(f32), pooling_group_matrix.astype(f32))
    pool_out = (grouped.reshape(row_total, POOL_WIDTH) * pooling_output_scale).astype(bf16)
    mix_cols = MIXER_CHANNELS // N_TP
    pool_cols = POOL_WIDTH // N_TP
    total = jnp.zeros((row_total, D), f32)
    for block in range(N_TP):
        term = jnp.dot(attn_out[:, block * mix_cols:(block + 1) * mix_cols], output_attention_rows[block * mix_cols:(block + 1) * mix_cols], preferred_element_type=f32)
        term = term + jnp.dot(pool_out[:, block * pool_cols:(block + 1) * pool_cols], output_pooling_rows[block * pool_cols:(block + 1) * pool_cols], preferred_element_type=f32)
        total = total + term.astype(bf16).astype(f32)
    return total.astype(bf16)
```

```python
import functools

import jax
import jax.numpy as jnp
from jax import lax
from jax.experimental import pallas as pl
from jax.experimental.pallas import tpu as pltpu
from jax.sharding import Mesh
from jax.sharding import PartitionSpec as P

Z = ("zh", "zl")
SP = ("zh", "zl", "y")
TP = ("x", "c")
f32 = jnp.float32
bf16 = jnp.bfloat16
HEAD = 64
CHUNK = 64
ROWS = 128
LANES = 128
PAY = 160
TAIL = 128
LEFT = 144
HIGHEST = lax.Precision.HIGHEST
NT = (((1,), (1,)), ((), ()))
TN = (((0,), (0,)), ((), ()))


def iota(shape, dim):
    return lax.broadcasted_iota(jnp.int32, shape, dim)


def mm(a, b, dims=(((1,), (0,)), ((), ()))):
    return lax.dot_general(a.astype(bf16), b.astype(bf16), dims, preferred_element_type=f32)


def mm32(a, b):
    return jnp.dot(a, b, preferred_element_type=f32, precision=HIGHEST)


def call(kernel, outs, *args, flops=10**8, name=None):
    size = sum(a.size * a.dtype.itemsize for a in args)
    return pl.pallas_call(
        kernel,
        out_shape=outs,
        in_specs=[pl.BlockSpec(memory_space=pltpu.VMEM)] * len(args),
        out_specs=jax.tree.map(lambda _: pl.BlockSpec(memory_space=pltpu.VMEM), outs),
        cost_estimate=pl.CostEstimate(flops=flops, bytes_accessed=size, transcendentals=0),
        name=name,
    )(*args)


def shaped(shape, dtype):
    return jax.ShapeDtypeStruct(shape, dtype)


def prepare_tokens(tok_ref, gain_ref, bias_ref, out_ref):
    wide = tok_ref[...].astype(f32)
    center = jnp.mean(wide, axis=-1, keepdims=True)
    off = wide - center
    spread = jnp.mean(jnp.square(off), axis=-1, keepdims=True)
    normed = (off * lax.rsqrt(spread + 1e-05) * gain_ref[...] + bias_ref[...]).astype(bf16)
    source = iota((512, 512), 0)
    target = iota((512, 512), 1)
    moved = ((source >> 5) & 3) * 128 + (source >> 7) * 32 + (source & 31)
    pick = jnp.where(moved == target, 1.0, 0.0).astype(bf16)
    for j in range(4):
        turned = jnp.dot(normed[:, 512 * j : 512 * j + 512], pick, preferred_element_type=f32)
        for y in range(4):
            out_ref[y, :, 128 * j : 128 * j + 128] = turned[:, 128 * y : 128 * y + 128].astype(bf16)


def prepare_weights(q_ref, k_ref, v_ref, p_ref, d_ref, r_ref, g_ref, oa_ref, op_ref, out_ref):
    first = lax.axis_index("c") == 0
    out_ref[:, 0:128] = q_ref[...]
    out_ref[:, 128:256] = k_ref[...]
    out_ref[:, 256:384] = v_ref[...]
    out_ref[:, 384:512] = p_ref[...]
    gate = g_ref[...]
    out_ref[:, 512:640] = jnp.where(first, d_ref[...], gate[:, :128])
    out_ref[:, 640:768] = jnp.where(first, r_ref[...], gate[:, 128:])
    out_ref[:, 768:896] = oa_ref[...].astype(f32).T.astype(bf16)
    out_ref[:, 896:1023] = op_ref[...].astype(f32).T.astype(bf16)[:, :127]


def partial_products(tok_ref, w_ref, part_ref, out_ref):
    made = jnp.dot(tok_ref[...], w_ref[:, :768], preferred_element_type=f32).astype(bf16)
    for y in range(4):
        part_ref[y] = made[128 * y : 128 * y + 128]
    first = w_ref[:, 768:896]
    second = w_ref[:, 896:1023]
    for y in range(4):
        out_ref[y, :, 0:128] = first
        out_ref[y, :, 128:255] = second
        out_ref[y, :, 255:256] = jnp.zeros((512, 1), bf16)


def sum_parts(part_ref, main_ref, low_ref):
    total = part_ref[0].astype(f32)
    for y in range(1, 4):
        total = total + part_ref[y].astype(f32)
    rounded = total.astype(bf16)
    main_ref[...] = rounded[:, :512]
    low = rounded[:, 512:].astype(f32)
    first = lax.axis_index("c") == 0
    one = jnp.where(first, jnp.tanh(low[:, :128]), jax.nn.sigmoid(low[:, :128]))
    two = jnp.where(first, low[:, 128:], jax.nn.sigmoid(low[:, 128:]))
    low_ref[:, :128] = one.astype(bf16)
    low_ref[:, 128:] = two.astype(bf16)


def by_head(lane_low, zero_head, one_head):
    return jnp.where(lane_low, zero_head, one_head)


def block_diagonal(pair):
    low = iota(pair.shape, 1) < HEAD
    zero = jnp.zeros_like(pair)
    return jnp.concatenate([jnp.where(low, pair, zero), jnp.where(low, zero, pair)], axis=0)


def recurrence(
    main_ref, low_ref, dw_ref, rw_ref, gw_ref, db_ref, lb_ref, kp_ref, kl_ref, st_ref,
    re_ref, de_ref, left_ref, pay_ref, ymap_ref, yloc_ref, gate_ref,
):
    recept = main_ref[:, 0:128].astype(f32)
    keys = main_ref[:, 128:256].astype(f32)
    values_b = main_ref[:, 256:384]
    values = values_b.astype(f32)
    row = iota((ROWS, LANES), 0)
    col = iota((ROWS, LANES), 1)
    lane_low = col < HEAD
    same = (row // CHUNK) == (col // CHUNK)

    drive = db_ref[...] + jnp.dot(low_ref[0, :, :128], dw_ref[...], preferred_element_type=f32)
    log_decay = -jax.nn.sigmoid(drive) * jnp.exp(re_ref[...] - 0.5) + de_ref[...]
    rate = jax.nn.sigmoid(
        lb_ref[...] + jnp.dot(low_ref[0, :, 128:], rw_ref[...], preferred_element_type=f32)
    )
    gate_ref[...] = jnp.dot(low_ref[1], gw_ref[...], preferred_element_type=f32)

    ones = jnp.where(same, 1.0, 0.0).astype(f32)
    unit = keys * kp_ref[...]
    effective = keys * (1.0 + (rate - 1.0) * kl_ref[...])
    sums = mm32(
        jnp.concatenate([unit * unit, recept * effective * st_ref[...]], axis=0), ones
    )
    unit = unit * lax.rsqrt(sums[:ROWS] + 1e-06)
    own = sums[ROWS:] * values
    beta = unit * rate

    tril = jnp.where(same & (row >= col), 1.0, 0.0).astype(f32)
    totals = mm32(jnp.concatenate([tril, ones], axis=0), log_decay)
    total, end = totals[:ROWS], totals[ROWS:]
    ref = 0.5 * end
    grow = jnp.exp(ref - total)
    shrink = jnp.exp(total - ref)
    base = jnp.exp(ref)
    a_hat = -unit * jnp.exp(total - log_decay - ref)
    r_hat = recept * shrink
    b_hat = beta * grow
    k_hat = effective * grow

    def masked(x):
        zero = jnp.zeros_like(x)
        return [jnp.where(lane_low, x, zero), jnp.where(lane_low, zero, x)]

    left = jnp.concatenate(masked(a_hat) + masked(r_hat), axis=0)
    right = jnp.concatenate([b_hat, k_hat], axis=0)
    scores = mm(left, right, NT)
    strict = same & (row > col)
    upto = same & (row >= col)

    def score(which, head, side, mask):
        at = (2 * which + head) * ROWS
        return jnp.where(mask, scores[at : at + ROWS, side * ROWS : side * ROWS + ROWS], 0.0)

    eye = jnp.where(row == col, 1.0, 0.0).astype(f32)
    within16 = (row // 16) == (col // 16)
    within32 = (row // 32) == (col // 32)
    a_start = a_hat * base
    swapped = pltpu.roll(a_start, HEAD, 1)
    solved, reads = [], []
    power, product = [], []
    full = [score(0, h, 0, strict) for h in range(2)]
    for h in range(2):
        power.append(jnp.where(within16, full[h], 0.0))
        product.append(eye + power[h])
    for _ in range(3):
        power = [mm32(power[h], power[h]) for h in range(2)]
        product = [product[h] + mm32(product[h], power[h]) for h in range(2)]
    step = [jnp.where(within32 & ~within16, full[h], 0.0) for h in range(2)]
    mid = [mm32(product[h], step[h]) for h in range(2)]
    product = [product[h] + mm32(mid[h], product[h]) for h in range(2)]
    step = [jnp.where(within32, 0.0, full[h]) for h in range(2)]
    mid = [mm32(product[h], step[h]) for h in range(2)]
    product = [product[h] + mm32(mid[h], product[h]) for h in range(2)]
    for h in range(2):
        pushed = mm(score(0, h, 1, strict), values_b)
        side = lane_low if h == 0 else ~lane_low
        rhs = jnp.where(side, pushed, swapped)
        solved.append(mm(product[h], rhs))
        reads.append(mm(score(1, h, 0, upto), solved[h]))
    direct = [mm(score(1, h, 1, upto), values_b) for h in range(2)]
    y_local = by_head(lane_low, reads[0], reads[1]) + by_head(lane_low, direct[0], direct[1])
    y_map = r_hat * base + pltpu.roll(by_head(lane_low, reads[1], reads[0]), HEAD, 1)

    b_end = (b_hat * base).astype(bf16)
    k_end = (k_hat * base).astype(bf16)
    decay_end = jnp.exp(end)
    low64 = iota((CHUNK, LANES), 1) < HEAD
    diagonal = iota((CHUNK, LANES), 0) == (iota((CHUNK, LANES), 1) % HEAD)
    maps, states = [], []
    for c in range(2):
        at = slice(c * CHUNK, c * CHUNK + CHUNK)
        g0 = mm(solved[0][at], b_end[at], TN)
        g1 = mm(solved[1][at], b_end[at], TN)
        kv = mm(values_b[at], k_end[at], TN)
        maps.append(
            jnp.where(diagonal, decay_end[at], 0.0)
            + by_head(low64, g0[HEAD:], g1[:HEAD])
        )
        states.append(
            by_head(low64, g0[:HEAD], g1[HEAD:]) + by_head(low64, kv[:HEAD], kv[HEAD:])
        )
    joined = mm(jnp.concatenate([maps[0], states[0]], axis=0), block_diagonal(maps[1]))
    block_map = joined[:CHUNK]
    block_state = joined[CHUNK:] + states[1]
    late = mm(
        y_map[CHUNK:],
        jnp.concatenate([block_diagonal(states[0]), block_diagonal(maps[0])], axis=0),
        NT,
    )
    ymap_ref[:CHUNK] = y_map[:CHUNK]
    ymap_ref[CHUNK:] = late[:, LANES:]
    yloc_ref[0, :CHUNK] = y_local[:CHUNK]
    yloc_ref[0, CHUNK:] = y_local[CHUNK:] + late[:, :LANES]
    yloc_ref[1] = own
    y = lax.axis_index("y")
    mine = jnp.where(col[:16] // 32 == y, left_ref[...].astype(f32), 0.0)
    mine = jnp.where(row[:16] == 0, mine, 0.0).astype(bf16)
    block_map = block_map.astype(bf16)
    block_state = block_state.astype(bf16)
    tail = main_ref[ROWS - 16 :, 384:512]
    for j in range(4):
        pay_ref[j, 0:64] = block_map
        pay_ref[j, 64:128] = block_state
        pay_ref[j, TAIL : TAIL + 16] = tail
        pay_ref[j, LEFT : LEFT + 16] = mine


def identity_pair():
    eye = iota((HEAD, LANES), 0) == (iota((HEAD, LANES), 1) % HEAD)
    return jnp.concatenate([jnp.where(eye, 1.0, 0.0).astype(f32), jnp.zeros((HEAD, LANES), f32)], 0)


def compose(earlier, later):
    moved = mm(earlier, block_diagonal(later[:HEAD]))
    return jnp.concatenate([moved[:HEAD], moved[HEAD:] + later[HEAD:]], axis=0)


def prefixes(got_ref, mine):
    pieces = [got_ref[j, :128].astype(f32) for j in range(4)]
    running = pieces[0]
    before = jnp.where(mine == 0, identity_pair(), pieces[0])
    for j in range(1, 4):
        running = compose(running, pieces[j])
        if j < 3:
            before = jnp.where(mine > j, running, before)
    return before, running


def tail_before(got_ref, mine):
    zero = jnp.zeros((16, LANES), f32)
    found = zero
    for j in range(3):
        found = jnp.where(mine == j + 1, got_ref[j, TAIL : TAIL + 16].astype(f32), found)
    return found


def stage_y(got_ref, pay_ref, before_ref, tail_ref):
    y = lax.axis_index("y")
    before, running = prefixes(got_ref, y)
    before_ref[...] = before
    tail_ref[...] = tail_before(got_ref, y)
    left = got_ref[0, LEFT : LEFT + 16].astype(f32)
    for j in range(1, 4):
        left = left + got_ref[j, LEFT : LEFT + 16].astype(f32)
    running = running.astype(bf16)
    left = left.astype(bf16)
    for j in range(4):
        pay_ref[j, 0:128] = running
        pay_ref[j, TAIL : TAIL + 16] = got_ref[3, TAIL : TAIL + 16]
        pay_ref[j, LEFT : LEFT + 16] = left


def stage_zl(got_ref, before_ref, tail_ref, pay_ref, out_before_ref, out_tail_ref):
    y = lax.axis_index("y")
    zl = lax.axis_index("zl")
    before, running = prefixes(got_ref, zl)
    out_before_ref[...] = compose(before, before_ref[...])
    out_tail_ref[...] = jnp.where(y == 0, tail_before(got_ref, zl), tail_ref[...])
    row = iota((16, LANES), 0)
    left = jnp.zeros((16, LANES), f32)
    for j in range(4):
        line = got_ref[j, LEFT : LEFT + 16].astype(f32)[0:1]
        left = jnp.where(row == j, line, left)
    running = running.astype(bf16)
    left = left.astype(bf16)
    for j in range(4):
        pay_ref[j, 0:128] = running
        pay_ref[j, TAIL : TAIL + 16] = got_ref[3, TAIL : TAIL + 16]
        pay_ref[j, LEFT : LEFT + 16] = left


def finish(
    got_ref, before_ref, tail_ref, start_ref, ymap_ref, yloc_ref, gate_ref, hs_ref, hb_ref,
    pool_ref, matrix_ref, scale_ref, wout_ref, out_ref,
):
    zh, zl, y = lax.axis_index("zh"), lax.axis_index("zl"), lax.axis_index("y")
    state = jnp.concatenate([start_ref[0], start_ref[1]], axis=1)
    for j in range(3):
        piece = got_ref[j, :128].astype(f32)
        state = jnp.where(zh > j, mm(state, block_diagonal(piece[:HEAD])) + piece[HEAD:], state)
    state = mm(state, block_diagonal(before_ref[:HEAD])) + before_ref[HEAD:]
    reading = yloc_ref[0] + mm(ymap_ref[...], block_diagonal(state), NT)
    row = iota((ROWS, LANES), 0)
    col = iota((ROWS, LANES), 1)
    mean = jnp.where((row // HEAD) == (col // HEAD), 1.0 / HEAD, 0.0).astype(f32)
    off = reading - mm32(reading, mean)
    spread = mm32(off * off, mean)
    headed = off * lax.rsqrt(spread + 1e-05 * HEAD) * hs_ref[...] + hb_ref[...] + yloc_ref[1]
    attn = (headed * gate_ref[...]).astype(bf16)

    pool = pool_ref[:, 384:512].astype(f32)
    tail = jnp.where((y == 0) & (zl == 0), tail_before(got_ref, zh), tail_ref[...])
    extended = jnp.concatenate([tail, pool], axis=0)
    level = lax.axis_index("x")
    sums = extended
    chosen = None
    for k in range(4):
        width = 1 << k
        shifted = pltpu.roll(sums, width, 0)
        sums = sums + jnp.where(iota(sums.shape, 0) < width, 0.0, shifted)
        picked = sums[16:]
        chosen = picked if k == 0 else jnp.where(level >= k, picked, chosen)
    window = lax.shift_left(jnp.int32(2), level).astype(f32)
    position = (((zh * 4 + zl) * 4 + y) * ROWS + row).astype(f32)
    pooled = (chosen / jnp.minimum(position + 1.0, window) - pool).astype(bf16)
    grouped = jnp.dot(pooled, matrix_ref[0], preferred_element_type=f32)
    pool_out = (grouped * scale_ref[...]).astype(bf16)

    acts = jnp.concatenate([attn, pool_out], axis=1)
    last = pool_out[:, 127:128].astype(f32)
    for zpair in range(8):
        rows = []
        for z in (2 * zpair, 2 * zpair + 1):
            for yy in range(4):
                rows.append(wout_ref[yy, 32 * z : 32 * z + 32])
        made = mm(acts, jnp.concatenate(rows, axis=0), NT)
        for half in range(2):
            z = 2 * zpair + half
            line = got_ref[z // 4, LEFT : LEFT + 16].astype(f32)[z % 4 : z % 4 + 1]
            out_ref[:, 128 * z : 128 * z + 128] = (
                made[:, 128 * half : 128 * half + 128] + last * line
            ).astype(bf16)


def on_device(
    tokens, input_norm_scale, input_norm_bias, query_projection, key_projection,
    value_projection, pooling_input_projection, decay_input_weight, rate_input_weight,
    gate_input_weight, decay_output_weight, rate_output_weight, gate_output_weight,
    decay_bias_base, learning_rate_base, key_prenorm_scale, key_learning_scale,
    self_term_weight, head_norm_scale, head_norm_bias, rate_extra_log, decay_extra_log,
    starting_head_state, pooling_group_matrix, pooling_output_scale, output_attention_rows,
    output_pooling_rows,
):
    line = lambda v: v.reshape(1, -1)
    sent = call(
        prepare_tokens, shaped((4, 128, 512), bf16),
        tokens, line(input_norm_scale), line(input_norm_bias), name="prepare_tokens",
    )
    shard = call(
        prepare_weights, shaped((32, 1023), bf16),
        query_projection, key_projection, value_projection, pooling_input_projection,
        decay_input_weight, rate_input_weight, gate_input_weight, output_attention_rows,
        output_pooling_rows, name="prepare_weights",
    )
    gathered = lax.all_gather(shard, Z, axis=0, tiled=True)
    mixed_tokens = lax.all_to_all(sent, "y", 0, 0, tiled=True).reshape(512, 512)
    parts, out_columns = call(
        partial_products,
        [shaped((4, 128, 768), bf16), shaped((4, 512, 256), bf16)],
        mixed_tokens, gathered, name="partial_products",
    )
    parts = lax.all_to_all(parts, "y", 0, 0, tiled=True)
    main, low = call(
        sum_parts, [shaped((128, 512), bf16), shaped((128, 256), bf16)], parts, name="sum_parts"
    )
    low = lax.all_gather(low, "c", axis=0)
    left = jnp.tile(output_pooling_rows[127:128], (1, 4))
    pay, y_map, y_local, gate = call(
        recurrence,
        [
            shaped((4, PAY, 128), bf16), shaped((128, 128), f32), shaped((2, 128, 128), f32),
            shaped((128, 128), f32),
        ],
        main, low, decay_output_weight, rate_output_weight, gate_output_weight,
        line(decay_bias_base), line(learning_rate_base), line(key_prenorm_scale),
        line(key_learning_scale), line(self_term_weight), rate_extra_log, decay_extra_log,
        left, name="recurrence",
    )
    out_columns = lax.all_to_all(out_columns, "y", 0, 0, tiled=True)
    got = lax.all_to_all(pay, "y", 0, 0, tiled=True)
    pay, before, tail = call(
        stage_y,
        [shaped((4, PAY, 128), bf16), shaped((128, 128), f32), shaped((16, 128), f32)],
        got, name="stage_y",
    )
    got = lax.all_to_all(pay, "zl", 0, 0, tiled=True)
    pay, before, tail = call(
        stage_zl,
        [shaped((4, PAY, 128), bf16), shaped((128, 128), f32), shaped((16, 128), f32)],
        got, before, tail, name="stage_zl",
    )
    got = lax.all_to_all(pay, "zh", 0, 0, tiled=True)
    out = call(
        finish, shaped((128, 2048), bf16),
        got, before, tail, starting_head_state, y_map, y_local, gate, line(head_norm_scale),
        line(head_norm_bias), main, pooling_group_matrix, line(pooling_output_scale),
        out_columns, name="finish",
    )
    parts = lax.all_to_all(out.reshape(8, 16, 2048), TP, 0, 0, tiled=True)
    return jnp.sum(parts.astype(f32), axis=0).astype(bf16)


def solution(mesh):
    split = Mesh(mesh.devices.reshape(4, 4, 4, 4, 2), ("zh", "zl", "y", "x", "c"))
    in_specs = (
        P(SP, None), P(), P(),
        P(SP, TP), P(SP, TP), P(SP, TP), P(SP, TP),
        P(SP, None), P(SP, None), P(SP, None),
        P(None, TP), P(None, TP), P(None, TP),
        P(TP), P(TP), P(TP), P(TP), P(TP), P(TP), P(TP),
        P(SP, TP), P(SP, TP),
        P(TP, None, None), P(TP, None, None), P(TP),
        P(TP, SP), P(TP, SP),
    )
    out_specs = P((*SP, *TP), None)
    return jax.shard_map(
        on_device, mesh=split, in_specs=in_specs, out_specs=out_specs, check_vma=False
    )
```

```python
import functools

import jax
import jax.numpy as jnp
from jax import lax
from jax.experimental import pallas as pl
from jax.experimental.pallas import tpu as pltpu
from jax.sharding import Mesh
from jax.sharding import PartitionSpec as P

Z = ("zh", "zl")
SP = ("zh", "zl", "y")
TP = ("x", "c")
f32 = jnp.float32
bf16 = jnp.bfloat16
HEAD = 64
CHUNK = 64
ROWS = 128
LANES = 128
PAY = 144
WIDE = 160
TAIL = 128
LEFT = 144
HIGHEST = lax.Precision.HIGHEST
NT = (((1,), (1,)), ((), ()))
TN = (((0,), (0,)), ((), ()))


def iota(shape, dim):
    return lax.broadcasted_iota(jnp.int32, shape, dim)


def mm(a, b, dims=(((1,), (0,)), ((), ()))):
    return lax.dot_general(a.astype(bf16), b.astype(bf16), dims, preferred_element_type=f32)


def mm32(a, b):
    return jnp.dot(a, b, preferred_element_type=f32, precision=HIGHEST)


def call(kernel, outs, *args, flops=10**8, name=None, vmem=16 * 2**20, space=pltpu.VMEM, scratch=()):
    size = sum(a.size * a.dtype.itemsize for a in args)
    return pl.pallas_call(
        kernel,
        out_shape=outs,
        in_specs=[pl.BlockSpec(memory_space=space)] * len(args),
        out_specs=jax.tree.map(lambda _: pl.BlockSpec(memory_space=pltpu.VMEM), outs),
        scratch_shapes=scratch,
        compiler_params=pltpu.CompilerParams(vmem_limit_bytes=vmem),
        cost_estimate=pl.CostEstimate(flops=flops, bytes_accessed=size, transcendentals=0),
        name=name,
    )(*args)


def shaped(shape, dtype):
    return jax.ShapeDtypeStruct(shape, dtype)


def prepare_tokens(tok_hbm, gain_hbm, bias_hbm, out_ref, tok, gain, bias, sems):
    halves = [
        pltpu.make_async_copy(
            tok_hbm.at[pl.ds(64 * i, 64)], tok.at[pl.ds(64 * i, 64)], sems.at[i]
        )
        for i in range(2)
    ]
    first = pltpu.make_async_copy(gain_hbm, gain, sems.at[2])
    second = pltpu.make_async_copy(bias_hbm, bias, sems.at[3])
    for copy in (halves[0], first, second, halves[1]):
        copy.start()
    source = iota((512, 512), 0)
    target = iota((512, 512), 1)
    moved = ((source >> 5) & 3) * 128 + (source >> 7) * 32 + (source & 31)
    pick = jnp.where(moved == target, 1.0, 0.0).astype(bf16)
    for i in range(2):
        halves[i].wait()
        if i == 0:
            first.wait()
            second.wait()
        rows = slice(64 * i, 64 * i + 64)
        wide = tok[rows].astype(f32)
        center = jnp.mean(wide, axis=-1, keepdims=True)
        off = wide - center
        spread = jnp.mean(jnp.square(off), axis=-1, keepdims=True)
        normed = (off * lax.rsqrt(spread + 1e-05) * gain[...] + bias[...]).astype(bf16)
        for j in range(4):
            turned = jnp.dot(normed[:, 512 * j : 512 * j + 512], pick, preferred_element_type=f32)
            turned = turned.astype(bf16)
            for y in range(4):
                out_ref[y, rows, 128 * j : 128 * j + 128] = turned[:, 128 * y : 128 * y + 128]


def prepare_weights(
    q_ref, k_ref, v_ref, p_ref, d_ref, r_ref, g_ref, oa_ref, op_ref, *rest
):
    *lines, out_ref, left_ref, lines_ref = rest
    for i, ref in enumerate(lines):
        lines_ref[i : i + 1] = ref[...]
    first = lax.axis_index("c") == 0
    out_ref[:, 0:128] = q_ref[...]
    out_ref[:, 128:256] = k_ref[...]
    out_ref[:, 256:384] = v_ref[...]
    out_ref[:, 384:512] = p_ref[...]
    gate = g_ref[...]
    out_ref[:, 512:640] = jnp.where(first, d_ref[...], gate[:, :128])
    out_ref[:, 640:768] = jnp.where(first, r_ref[...], gate[:, 128:])
    out_ref[:, 768:896] = oa_ref[...]
    out_ref[:, 896:1023] = op_ref[:, :127]
    spot = iota((32, LANES), 1) == lax.axis_index("y") * 32 + iota((32, LANES), 0)
    column = op_ref[...].astype(f32)[:, 127:128]
    line = jnp.sum(jnp.where(spot, column, 0.0), axis=0, keepdims=True)
    left_ref[...] = jnp.where(iota((16, LANES), 0) == 0, line, 0.0)


def partial_products(tok_ref, w_ref, part_ref):
    made = jnp.dot(tok_ref[...], w_ref[:, :768], preferred_element_type=f32).astype(bf16)
    for y in range(4):
        part_ref[y] = made[128 * y : 128 * y + 128]


def spread_columns(w_ref, out_ref):
    first = w_ref[:, 768:896]
    second = w_ref[:, 896:1023]
    for y in range(4):
        out_ref[y, :, 0:128] = first
        out_ref[y, :, 128:255] = second
        out_ref[y, :, 255:256] = jnp.zeros((512, 1), bf16)


def sum_parts(part_ref, main_ref, low_ref):
    total = part_ref[0].astype(f32)
    for y in range(1, 4):
        total = total + part_ref[y].astype(f32)
    rounded = total.astype(bf16)
    main_ref[...] = rounded[:, :512]
    low = rounded[:, 512:].astype(f32)
    first = lax.axis_index("c") == 0
    one = jnp.where(first, jnp.tanh(low[:, :128]), jax.nn.sigmoid(low[:, :128]))
    two = jnp.where(first, low[:, 128:], jax.nn.sigmoid(low[:, 128:]))
    low_ref[:, :128] = one.astype(bf16)
    low_ref[:, 128:] = two.astype(bf16)


def masked(x, lane_low):
    zero = jnp.zeros_like(x)
    return [jnp.where(lane_low, x, zero), jnp.where(lane_low, zero, x)]


def block_diagonal(pair):
    low = iota(pair.shape, 1) < HEAD
    zero = jnp.zeros_like(pair)
    return jnp.concatenate([jnp.where(low, pair, zero), jnp.where(low, zero, pair)], axis=0)


def block_maps(
    main_ref, low_ref, dw_ref, rw_ref, lines_ref, re_ref, de_ref, left_ref, pay_ref, solved_ref, hats_ref, first_ref, wide_ref,
):
    line = lambda i: lines_ref[i : i + 1]
    recept = main_ref[:, 0:128].astype(f32)
    keys = main_ref[:, 128:256].astype(f32)
    values_b = main_ref[:, 256:384]
    values = values_b.astype(f32)
    row = iota((ROWS, LANES), 0)
    col = iota((ROWS, LANES), 1)
    lane_low = col < HEAD
    same = (row // CHUNK) == (col // CHUNK)

    drive = line(0) + jnp.dot(low_ref[0, :, :128], dw_ref[...], preferred_element_type=f32)
    log_decay = -jax.nn.sigmoid(drive) * jnp.exp(re_ref[...] - 0.5) + de_ref[...]
    rate = jax.nn.sigmoid(
        line(1) + jnp.dot(low_ref[0, :, 128:], rw_ref[...], preferred_element_type=f32)
    )

    ones = jnp.where(same, 1.0, 0.0).astype(f32)
    unit = keys * line(2)
    effective = keys * (1.0 + (rate - 1.0) * line(3))
    sums = mm32(
        jnp.concatenate([unit * unit, recept * effective * line(4)], axis=0), ones
    )
    unit = unit * lax.rsqrt(sums[:ROWS] + 1e-06)
    wide_ref[1] = sums[ROWS:] * values
    beta = unit * rate

    tril = jnp.where(same & (row >= col), 1.0, 0.0).astype(f32)
    totals = mm32(jnp.concatenate([tril, ones], axis=0), log_decay)
    total, end = totals[:ROWS], totals[ROWS:]
    ref = 0.5 * end
    grow = jnp.exp(ref - total)
    shrink = jnp.exp(total - ref)
    base = jnp.exp(ref)
    a_hat = -unit * jnp.exp(total - log_decay - ref)
    r_hat = recept * shrink
    b_hat = beta * grow
    k_hat = effective * grow
    wide_ref[0] = r_hat * base
    hats_ref[0] = r_hat.astype(bf16)
    hats_ref[1] = b_hat.astype(bf16)
    hats_ref[2] = k_hat.astype(bf16)

    left = jnp.concatenate(masked(a_hat, lane_low), axis=0)
    right = jnp.concatenate([b_hat, k_hat], axis=0)
    scores = mm(left, right, NT)
    strict = same & (row > col)
    eye = jnp.where(row == col, 1.0, 0.0).astype(f32)
    within16 = (row // 16) == (col // 16)
    within32 = (row // 32) == (col // 32)
    swapped = pltpu.roll(a_hat * base, HEAD, 1)
    full = [jnp.where(strict, scores[h * ROWS : h * ROWS + ROWS, :ROWS], 0.0) for h in range(2)]
    power = [jnp.where(within16, full[h], 0.0) for h in range(2)]
    product = [eye + power[h] for h in range(2)]
    for _ in range(3):
        power = [mm32(power[h], power[h]) for h in range(2)]
        product = [product[h] + mm32(product[h], power[h]) for h in range(2)]
    for step in (
        [jnp.where(within32 & ~within16, full[h], 0.0) for h in range(2)],
        [jnp.where(within32, 0.0, full[h]) for h in range(2)],
    ):
        mid = [mm32(product[h], step[h]) for h in range(2)]
        product = [product[h] + mm32(mid[h], product[h]) for h in range(2)]
    solved = []
    for h in range(2):
        pushed = mm(jnp.where(strict, scores[h * ROWS : h * ROWS + ROWS, ROWS:], 0.0), values_b)
        rhs = jnp.where(lane_low if h == 0 else ~lane_low, pushed, swapped)
        solved.append(mm(product[h], rhs).astype(bf16))
        solved_ref[h] = solved[h]

    b_end = (b_hat * base).astype(bf16)
    k_end = (k_hat * base).astype(bf16)
    decay_end = jnp.exp(end)
    low64 = iota((CHUNK, LANES), 1) < HEAD
    diagonal = iota((CHUNK, LANES), 0) == (iota((CHUNK, LANES), 1) % HEAD)
    maps, states = [], []
    for c in range(2):
        at = slice(c * CHUNK, c * CHUNK + CHUNK)
        g0 = mm(solved[0][at], b_end[at], TN)
        g1 = mm(solved[1][at], b_end[at], TN)
        kv = mm(values_b[at], k_end[at], TN)
        maps.append(
            jnp.where(diagonal, decay_end[at], 0.0) + jnp.where(low64, g0[HEAD:], g1[:HEAD])
        )
        states.append(
            jnp.where(low64, g0[:HEAD], g1[HEAD:]) + jnp.where(low64, kv[:HEAD], kv[HEAD:])
        )
    chunk0 = jnp.concatenate([maps[0], states[0]], axis=0).astype(bf16)
    first_ref[...] = chunk0
    joined = mm(chunk0, block_diagonal(maps[1]))
    block_map = joined[:CHUNK].astype(bf16)
    block_state = (joined[CHUNK:] + states[1]).astype(bf16)
    tail = main_ref[ROWS - 16 :, 384:512].astype(f32)
    extra = jnp.where(row[:16] == 0, left_ref[...], tail).astype(bf16)
    for j in range(4):
        pay_ref[j, 0:64] = block_map
        pay_ref[j, 64:128] = block_state
        pay_ref[j, TAIL : TAIL + 16] = extra


def block_readings(main_ref, low_ref, gw_ref, solved_ref, hats_ref, first_ref, wide_ref, ymap_ref, out_ref):
    values_b = main_ref[:, 256:384]
    row = iota((ROWS, LANES), 0)
    col = iota((ROWS, LANES), 1)
    lane_low = col < HEAD
    upto = ((row // CHUNK) == (col // CHUNK)) & (row >= col)
    out_ref[1] = wide_ref[1]
    out_ref[2] = jnp.dot(low_ref[1], gw_ref[...], preferred_element_type=f32)
    scores = mm(
        jnp.concatenate(masked(hats_ref[0].astype(f32), lane_low), axis=0),
        jnp.concatenate([hats_ref[1], hats_ref[2]], axis=0),
        NT,
    )
    reads, direct = [], []
    for h in range(2):
        at = slice(h * ROWS, h * ROWS + ROWS)
        reads.append(mm(jnp.where(upto, scores[at, :ROWS], 0.0), solved_ref[h]))
        direct.append(mm(jnp.where(upto, scores[at, ROWS:], 0.0), values_b))
    y_local = jnp.where(lane_low, reads[0] + direct[0], reads[1] + direct[1])
    y_map = wide_ref[0] + pltpu.roll(jnp.where(lane_low, reads[1], reads[0]), HEAD, 1)
    first = first_ref[...].astype(f32)
    late = mm(
        y_map[CHUNK:],
        jnp.concatenate([block_diagonal(first[CHUNK:]), block_diagonal(first[:CHUNK])], axis=0),
        NT,
    )
    ymap_ref[:CHUNK] = y_map[:CHUNK].astype(bf16)
    ymap_ref[CHUNK:] = late[:, LANES:].astype(bf16)
    out_ref[0, :CHUNK] = y_local[:CHUNK]
    out_ref[0, CHUNK:] = y_local[CHUNK:] + late[:, :LANES]


def identity_pair():
    eye = iota((HEAD, LANES), 0) == (iota((HEAD, LANES), 1) % HEAD)
    return jnp.concatenate([jnp.where(eye, 1.0, 0.0).astype(f32), jnp.zeros((HEAD, LANES), f32)], 0)


def compose(earlier, later):
    moved = mm(earlier, block_diagonal(later[:HEAD]))
    return jnp.concatenate([moved[:HEAD], moved[HEAD:] + later[HEAD:]], axis=0)


def chain(first, others):
    made = [first]
    for other in others:
        made.append(compose(made[-1], other))
    return made


def chosen_before(made, mine):
    before = jnp.where(mine == 0, identity_pair(), made[0])
    for j in (1, 2):
        before = jnp.where(mine > j, made[j], before)
    return before


def tail_before(got_ref, mine):
    found = jnp.zeros((16, LANES), f32)
    for j in range(3):
        found = jnp.where(mine == j + 1, got_ref[j, TAIL : TAIL + 16].astype(f32), found)
    return found


def prefixes(got_ref, mine):
    pieces = [got_ref[j, :128].astype(f32) for j in range(4)]
    made = chain(pieces[0], pieces[1:])
    return chosen_before(made, mine), made[3].astype(bf16)


def stage_y(got_ref, pay_ref, before_ref, tail_ref):
    y = lax.axis_index("y")
    before, running = prefixes(got_ref, y)
    before_ref[...] = before
    tail_ref[...] = tail_before(got_ref, y)
    extras = [got_ref[j, TAIL : TAIL + 16].astype(f32) for j in range(4)]
    line = extras[0] + extras[1] + extras[2] + extras[3]
    extra = jnp.where(iota((16, LANES), 0) == 0, line, extras[3]).astype(bf16)
    for j in range(4):
        pay_ref[j, 0:128] = running
        pay_ref[j, TAIL : TAIL + 16] = extra


def stage_zl(got_ref, before_ref, tail_ref, pay_ref, out_before_ref, out_tail_ref):
    y, zl = lax.axis_index("y"), lax.axis_index("zl")
    before, running = prefixes(got_ref, zl)
    out_before_ref[...] = compose(before, before_ref[...])
    out_tail_ref[...] = jnp.where(y == 0, tail_before(got_ref, zl), tail_ref[...])
    row = iota((16, LANES), 0)
    left = jnp.zeros((16, LANES), f32)
    for j in range(4):
        left = jnp.where(row == j, got_ref[j, TAIL : TAIL + 16].astype(f32)[0:1], left)
    pay_ref[0:128] = running
    pay_ref[TAIL : TAIL + 16] = got_ref[3, TAIL : TAIL + 16]
    pay_ref[LEFT : LEFT + 16] = left.astype(bf16)


def finish(
    got_ref, before_ref, tail_ref, start_ref, ymap_ref, yloc_ref, lines_ref,
    pool_ref, matrix_ref, wout_ref, out_ref,
):
    zh, zl, y = lax.axis_index("zh"), lax.axis_index("zl"), lax.axis_index("y")
    state = jnp.concatenate([start_ref[0], start_ref[1]], axis=1)
    for j in range(3):
        piece = got_ref[j, :128].astype(f32)
        state = jnp.where(zh > j, mm(state, block_diagonal(piece[:HEAD])) + piece[HEAD:], state)
    state = mm(state, block_diagonal(before_ref[:HEAD])) + before_ref[HEAD:]
    reading = yloc_ref[0] + mm(ymap_ref[...], block_diagonal(state), NT)
    row = iota((ROWS, LANES), 0)
    col = iota((ROWS, LANES), 1)
    mean = jnp.where((row // HEAD) == (col // HEAD), 1.0 / HEAD, 0.0).astype(f32)
    off = reading - mm32(reading, mean)
    spread = mm32(off * off, mean)
    headed = off * lax.rsqrt(spread + 1e-05 * HEAD) * lines_ref[5:6] + lines_ref[6:7] + yloc_ref[1]
    attn = (headed * yloc_ref[2]).astype(bf16)

    pool = pool_ref[:, 384:512].astype(f32)
    tail = jnp.where((y == 0) & (zl == 0), tail_before(got_ref, zh), tail_ref[...])
    extended = jnp.concatenate([tail, pool], axis=0)
    level = lax.axis_index("x")
    sums = extended
    chosen = None
    for k in range(4):
        width = 1 << k
        shifted = pltpu.roll(sums, width, 0)
        sums = sums + jnp.where(iota(sums.shape, 0) < width, 0.0, shifted)
        picked = sums[16:]
        chosen = picked if k == 0 else jnp.where(level >= k, picked, chosen)
    window = lax.shift_left(jnp.int32(2), level).astype(f32)
    position = (((zh * 4 + zl) * 4 + y) * ROWS + row).astype(f32)
    pooled = (chosen / jnp.minimum(position + 1.0, window) - pool).astype(bf16)
    grouped = jnp.dot(pooled, matrix_ref[0], preferred_element_type=f32)
    pool_out = (grouped * lines_ref[7:8]).astype(bf16)

    acts = jnp.concatenate([attn, pool_out], axis=1)
    last = pool_out[:, 127:128].astype(f32)
    for zpair in range(8):
        rows = []
        for z in (2 * zpair, 2 * zpair + 1):
            for yy in range(4):
                rows.append(wout_ref[yy, 32 * z : 32 * z + 32])
        made = mm(acts, jnp.concatenate(rows, axis=0), NT)
        for half in range(2):
            z = 2 * zpair + half
            line = got_ref[z // 4, LEFT : LEFT + 16].astype(f32)[z % 4 : z % 4 + 1]
            out_ref[:, 128 * z : 128 * z + 128] = (
                made[:, 128 * half : 128 * half + 128] + last * line
            ).astype(bf16)


def add_parts(part_ref, out_ref):
    total = part_ref[0].astype(f32)
    for j in range(1, 8):
        total = total + part_ref[j].astype(f32)
    out_ref[...] = total.astype(bf16)


def on_device(
    tokens, input_norm_scale, input_norm_bias, query_projection, key_projection,
    value_projection, pooling_input_projection, decay_input_weight, rate_input_weight,
    gate_input_weight, decay_output_weight, rate_output_weight, gate_output_weight,
    decay_bias_base, learning_rate_base, key_prenorm_scale, key_learning_scale,
    self_term_weight, head_norm_scale, head_norm_bias, rate_extra_log, decay_extra_log,
    starting_head_state, pooling_group_matrix, pooling_output_scale, output_attention_rows,
    output_pooling_rows,
):
    line = lambda v: v.reshape(1, -1)
    sent = call(
        prepare_tokens, shaped((4, 128, 512), bf16),
        tokens, line(input_norm_scale), line(input_norm_bias), name="prepare_tokens",
        space=pltpu.HBM, vmem=60 * 2**20,
        scratch=[
            pltpu.VMEM((128, 2048), bf16), pltpu.VMEM((1, 2048), f32), pltpu.VMEM((1, 2048), f32),
            pltpu.SemaphoreType.DMA((4,)),
        ],
    )
    shard, left, lines = call(
        prepare_weights,
        [shaped((32, 1023), bf16), shaped((16, 128), f32), shaped((8, 128), f32)],
        query_projection, key_projection, value_projection, pooling_input_projection,
        decay_input_weight, rate_input_weight, gate_input_weight, output_attention_rows.T,
        output_pooling_rows.T, line(decay_bias_base), line(learning_rate_base),
        line(key_prenorm_scale), line(key_learning_scale), line(self_term_weight),
        line(head_norm_scale), line(head_norm_bias), line(pooling_output_scale),
        name="prepare_weights",
    )
    gathered = lax.all_gather(shard, Z, axis=0, tiled=True)
    mixed_tokens = lax.all_to_all(sent, "y", 0, 0, tiled=True).reshape(512, 512)
    parts = call(
        partial_products, shaped((4, 128, 768), bf16), mixed_tokens, gathered,
        name="partial_products",
    )
    parts = lax.all_to_all(parts, "y", 0, 0, tiled=True)
    main, low = call(
        sum_parts, [shaped((128, 512), bf16), shaped((128, 256), bf16)], parts, name="sum_parts"
    )
    low = lax.all_gather(low, "c", axis=0)
    pay, solved, hats, first, wide = call(
        block_maps,
        [
            shaped((4, PAY, 128), bf16), shaped((2, 128, 128), bf16), shaped((3, 128, 128), bf16),
            shaped((128, 128), bf16), shaped((2, 128, 128), f32),
        ],
        main, low, decay_output_weight, rate_output_weight, lines, rate_extra_log,
        decay_extra_log, left, name="block_maps",
    )
    columns, pay = lax.optimization_barrier((gathered, pay))
    got = lax.all_to_all(pay, "y", 0, 0, tiled=True)
    y_map, y_local = call(
        block_readings, [shaped((128, 128), bf16), shaped((3, 128, 128), f32)],
        main, low, gate_output_weight, solved, hats, first, wide, name="block_readings",
    )
    columns = call(spread_columns, shaped((4, 512, 256), bf16), columns, name="spread_columns")
    pay, before, tail = call(
        stage_y,
        [shaped((4, PAY, 128), bf16), shaped((128, 128), f32), shaped((16, 128), f32)],
        got, name="stage_y",
    )
    got = lax.all_to_all(pay, "zl", 0, 0, tiled=True)
    columns, got = lax.optimization_barrier((columns, got))
    columns = lax.all_to_all(columns, "y", 0, 0, tiled=True)
    pay, before, tail = call(
        stage_zl,
        [shaped((WIDE, 128), bf16), shaped((128, 128), f32), shaped((16, 128), f32)],
        got, before, tail, name="stage_zl",
    )
    got = lax.all_gather(pay, "zh", axis=0)
    out = call(
        finish, shaped((128, 2048), bf16),
        got, before, tail, starting_head_state, y_map, y_local, lines, main,
        pooling_group_matrix, columns, name="finish",
    )
    parts = lax.all_to_all(out.reshape(8, 16, 2048), TP, 0, 0, tiled=True)
    return call(add_parts, shaped((16, 2048), bf16), parts, name="add_parts")


def solution(mesh):
    split = Mesh(mesh.devices.reshape(4, 4, 4, 4, 2), ("zh", "zl", "y", "x", "c"))
    in_specs = (
        P(SP, None), P(), P(),
        P(SP, TP), P(SP, TP), P(SP, TP), P(SP, TP),
        P(SP, None), P(SP, None), P(SP, None),
        P(None, TP), P(None, TP), P(None, TP),
        P(TP), P(TP), P(TP), P(TP), P(TP), P(TP), P(TP),
        P(SP, TP), P(SP, TP),
        P(TP, None, None), P(TP, None, None), P(TP),
        P(TP, SP), P(TP, SP),
    )
    out_specs = P((*SP, *TP), None)
    return jax.shard_map(
        on_device, mesh=split, in_specs=in_specs, out_specs=out_specs, check_vma=False
    )
```

```python
import functools

import jax
import jax.numpy as jnp
from jax import lax
from jax.experimental import pallas as pl
from jax.experimental.pallas import tpu as pltpu
from jax.sharding import Mesh
from jax.sharding import PartitionSpec as P

Z = ("zh", "zl")
SP = ("zh", "zl", "y")
TP = ("x", "c")
f32 = jnp.float32
bf16 = jnp.bfloat16
HEAD = 64
CHUNK = 64
ROWS = 128
LANES = 128
PAY = 144
WIDE = 160
TAIL = 128
LEFT = 144
NT = (((1,), (1,)), ((), ()))
TN = (((0,), (0,)), ((), ()))


def iota(shape, dim):
    return lax.broadcasted_iota(jnp.int32, shape, dim)


def mm(a, b, dims=(((1,), (0,)), ((), ()))):
    return lax.dot_general(a.astype(bf16), b.astype(bf16), dims, preferred_element_type=f32)


def split(x, parts):
    found = []
    for _ in range(parts):
        piece = x.astype(bf16)
        found.append(piece)
        x = x - piece.astype(f32)
    return found


def mm_exact_right(x, exact):
    return jnp.dot(
        jnp.concatenate(split(x, 3), axis=1),
        jnp.concatenate([exact] * 3, axis=0),
        preferred_element_type=f32,
    )


def mm_exact_left(exact, x):
    return jnp.dot(
        jnp.concatenate([exact] * 3, axis=1),
        jnp.concatenate(split(x, 3), axis=0),
        preferred_element_type=f32,
    )


def mm_wide(a, b):
    a0, a1 = split(a, 2)
    b0, b1 = split(b, 2)
    return jnp.dot(
        jnp.concatenate([a0, a0, a1], axis=1),
        jnp.concatenate([b0, b1, b0], axis=0),
        preferred_element_type=f32,
    )


def call(kernel, outs, *args, flops=10**8, name=None, vmem=16 * 2**20, space=pltpu.VMEM, scratch=()):
    size = sum(a.size * a.dtype.itemsize for a in args)
    return pl.pallas_call(
        kernel,
        out_shape=outs,
        in_specs=[pl.BlockSpec(memory_space=space)] * len(args),
        out_specs=jax.tree.map(lambda _: pl.BlockSpec(memory_space=pltpu.VMEM), outs),
        scratch_shapes=scratch,
        compiler_params=pltpu.CompilerParams(vmem_limit_bytes=vmem),
        cost_estimate=pl.CostEstimate(flops=flops, bytes_accessed=size, transcendentals=0),
        name=name,
    )(*args)


def shaped(shape, dtype):
    return jax.ShapeDtypeStruct(shape, dtype)


def prepare_tokens(tok_hbm, gain_hbm, bias_hbm, *rest):
    *vectors, out_ref, lines_ref, tok, gain, bias, sems = rest
    lines = [
        pltpu.make_async_copy(ref, lines_ref.at[pl.ds(i, 1)], sems.at[3 + i])
        for i, ref in enumerate(vectors)
    ]
    copies = [
        pltpu.make_async_copy(tok_hbm, tok, sems.at[0]),
        pltpu.make_async_copy(gain_hbm, gain, sems.at[1]),
        pltpu.make_async_copy(bias_hbm, bias, sems.at[2]),
        *lines,
    ]
    for copy in copies:
        copy.start()
    source = iota((512, 512), 0)
    target = iota((512, 512), 1)
    moved = ((source >> 5) & 3) * 128 + (source >> 7) * 32 + (source & 31)
    pick = jnp.where(moved == target, 1.0, 0.0).astype(bf16)
    for copy in copies:
        copy.wait()
    wide = tok[...].astype(f32)
    center = jnp.mean(wide, axis=-1, keepdims=True)
    off = wide - center
    spread = jnp.mean(jnp.square(off), axis=-1, keepdims=True)
    normed = (off * lax.rsqrt(spread + 1e-05) * gain[...] + bias[...]).astype(bf16)
    for j in range(4):
        turned = jnp.dot(normed[:, 512 * j : 512 * j + 512], pick, preferred_element_type=f32)
        for y in range(4):
            out_ref[y, :, 128 * j : 128 * j + 128] = turned[:, 128 * y : 128 * y + 128].astype(bf16)


def prepare_weights(
    q_ref, k_ref, v_ref, p_ref, d_ref, r_ref, g_ref, oa_ref, op_ref, out_ref, left_ref
):
    first = lax.axis_index("c") == 0
    out_ref[:, 0:128] = q_ref[...]
    out_ref[:, 128:256] = k_ref[...]
    out_ref[:, 256:384] = v_ref[...]
    out_ref[:, 384:512] = p_ref[...]
    gate = g_ref[...]
    out_ref[:, 512:640] = jnp.where(first, d_ref[...], gate[:, :128])
    out_ref[:, 640:768] = jnp.where(first, r_ref[...], gate[:, 128:])
    out_ref[:, 768:896] = oa_ref[...]
    out_ref[:, 896:1023] = op_ref[:, :127]
    spot = iota((32, LANES), 1) == lax.axis_index("y") * 32 + iota((32, LANES), 0)
    column = op_ref[...].astype(f32)[:, 127:128]
    line = jnp.sum(jnp.where(spot, column, 0.0), axis=0, keepdims=True)
    left_ref[...] = jnp.where(iota((16, LANES), 0) == 0, line, 0.0)


def partial_products(tok_ref, w_ref, part_ref):
    made = jnp.dot(tok_ref[...], w_ref[:, :768], preferred_element_type=f32).astype(bf16)
    for y in range(4):
        part_ref[y] = made[128 * y : 128 * y + 128]


def spread_columns(w_ref, out_ref):
    first = w_ref[:, 768:896]
    second = w_ref[:, 896:1023]
    for y in range(4):
        out_ref[y, :, 0:128] = first
        out_ref[y, :, 128:255] = second
        out_ref[y, :, 255:256] = jnp.zeros((512, 1), bf16)


def sum_parts(part_ref, main_ref, low_ref):
    total = part_ref[0].astype(f32)
    for y in range(1, 4):
        total = total + part_ref[y].astype(f32)
    rounded = total.astype(bf16)
    main_ref[...] = rounded[:, :512]
    low = rounded[:, 512:].astype(f32)
    first = lax.axis_index("c") == 0
    one = jnp.where(first, jnp.tanh(low[:, :128]), jax.nn.sigmoid(low[:, :128]))
    two = jnp.where(first, low[:, 128:], jax.nn.sigmoid(low[:, 128:]))
    low_ref[:, :128] = one.astype(bf16)
    low_ref[:, 128:] = two.astype(bf16)


def masked(x, lane_low):
    zero = jnp.zeros_like(x)
    return [jnp.where(lane_low, x, zero), jnp.where(lane_low, zero, x)]


def block_diagonal(pair):
    low = iota(pair.shape, 1) < HEAD
    zero = jnp.zeros_like(pair)
    return jnp.concatenate([jnp.where(low, pair, zero), jnp.where(low, zero, pair)], axis=0)


def block_maps(
    main_ref, low_ref, dw_ref, rw_ref, lines_ref, re_ref, de_ref, left_ref, pay_ref, solved_ref, hats_ref, first_ref, wide_ref,
):
    line = lambda i: lines_ref[i : i + 1]
    recept = main_ref[:, 0:128].astype(f32)
    keys = main_ref[:, 128:256].astype(f32)
    values_b = main_ref[:, 256:384]
    row = iota((ROWS, LANES), 0)
    col = iota((ROWS, LANES), 1)
    lane_low = col < HEAD
    same = (row // CHUNK) == (col // CHUNK)

    drive = line(0) + jnp.dot(low_ref[0, :, :128], dw_ref[...], preferred_element_type=f32)
    log_decay = -jax.nn.sigmoid(drive) * jnp.exp(re_ref[...] - 0.5) + de_ref[...]
    rate = jax.nn.sigmoid(
        line(1) + jnp.dot(low_ref[0, :, 128:], rw_ref[...], preferred_element_type=f32)
    )

    ones = jnp.where(same, 1.0, 0.0).astype(bf16)
    unit = keys * line(2)
    effective = keys * (1.0 + (rate - 1.0) * line(3))
    unit = unit * lax.rsqrt(mm_exact_right(unit * unit, ones) + 1e-06)
    wide_ref[1] = recept * effective
    beta = unit * rate

    tril = jnp.where(same & (row >= col), 1.0, 0.0).astype(bf16)
    totals = mm_exact_left(jnp.concatenate([tril, ones], axis=0), log_decay)
    total, end = totals[:ROWS], totals[ROWS:]
    ref = 0.5 * end
    grow = jnp.exp(ref - total)
    shrink = jnp.exp(total - ref)
    base = jnp.exp(ref)
    a_hat = -unit * jnp.exp(total - log_decay - ref)
    r_hat = recept * shrink
    b_hat = beta * grow
    k_hat = effective * grow
    wide_ref[0] = r_hat * base
    hats_ref[0] = r_hat.astype(bf16)
    hats_ref[1] = b_hat.astype(bf16)
    hats_ref[2] = k_hat.astype(bf16)

    left = jnp.concatenate(masked(a_hat, lane_low), axis=0)
    right = jnp.concatenate([b_hat, k_hat], axis=0)
    scores = mm(left, right, NT)
    strict = same & (row > col)
    eye = jnp.where(row == col, 1.0, 0.0).astype(f32)
    swapped = pltpu.roll(a_hat * base, HEAD, 1)
    full = [jnp.where(strict, scores[h * ROWS : h * ROWS + ROWS, :ROWS], 0.0) for h in range(2)]
    within = {n: (row // n) == (col // n) for n in (8, 16, 32)}
    power = [jnp.where(within[8], full[h], 0.0) for h in range(2)]
    product = [eye + power[h] for h in range(2)]
    for _ in range(2):
        power = [mm_wide(power[h], power[h]) for h in range(2)]
        product = [product[h] + mm_wide(product[h], power[h]) for h in range(2)]
    for here in (within[16] & ~within[8], within[32] & ~within[16], ~within[32]):
        mid = [mm_wide(product[h], jnp.where(here, full[h], 0.0)) for h in range(2)]
        product = [product[h] + mm_wide(mid[h], product[h]) for h in range(2)]
    solved = []
    for h in range(2):
        pushed = mm(jnp.where(strict, scores[h * ROWS : h * ROWS + ROWS, ROWS:], 0.0), values_b)
        rhs = jnp.where(lane_low if h == 0 else ~lane_low, pushed, swapped)
        solved.append(mm(product[h], rhs).astype(bf16))
        solved_ref[h] = solved[h]

    b_end = (b_hat * base).astype(bf16)
    k_end = (k_hat * base).astype(bf16)
    decay_end = jnp.exp(end)
    low64 = iota((CHUNK, LANES), 1) < HEAD
    diagonal = iota((CHUNK, LANES), 0) == (iota((CHUNK, LANES), 1) % HEAD)
    maps, states = [], []
    for c in range(2):
        at = slice(c * CHUNK, c * CHUNK + CHUNK)
        g0 = mm(solved[0][at], b_end[at], TN)
        g1 = mm(solved[1][at], b_end[at], TN)
        kv = mm(values_b[at], k_end[at], TN)
        maps.append(
            jnp.where(diagonal, decay_end[at], 0.0) + jnp.where(low64, g0[HEAD:], g1[:HEAD])
        )
        states.append(
            jnp.where(low64, g0[:HEAD], g1[HEAD:]) + jnp.where(low64, kv[:HEAD], kv[HEAD:])
        )
    chunk0 = jnp.concatenate([maps[0], states[0]], axis=0).astype(bf16)
    first_ref[...] = chunk0
    joined = mm(chunk0, block_diagonal(maps[1]))
    block_map = joined[:CHUNK].astype(bf16)
    block_state = (joined[CHUNK:] + states[1]).astype(bf16)
    tail = main_ref[ROWS - 16 :, 384:512].astype(f32)
    extra = jnp.where(row[:16] == 0, left_ref[...], tail).astype(bf16)
    for j in range(4):
        pay_ref[j, 0:64] = block_map
        pay_ref[j, 64:128] = block_state
        pay_ref[j, TAIL : TAIL + 16] = extra


def pool_rows(extended, own, place, matrix, scale):
    level = lax.axis_index("x")
    sums = extended
    chosen = None
    for k in range(4):
        width = 1 << k
        sums = sums + pltpu.roll(sums, width, 0)
        picked = sums[16:]
        chosen = picked if k == 0 else jnp.where(level >= k, picked, chosen)
    window = lax.shift_left(jnp.int32(2), level).astype(f32)
    position = (place + iota(own.shape, 0)).astype(f32)
    pooled = (chosen / jnp.minimum(position + 1.0, window) - own).astype(bf16)
    return jnp.dot(pooled, matrix, preferred_element_type=f32) * scale


def block_readings(
    main_ref, low_ref, gw_ref, solved_ref, hats_ref, first_ref, wide_ref, lines_ref, matrix_ref,
    ymap_ref, out_ref, pool_ref,
):
    pool = main_ref[:, 384:512].astype(f32)
    place = ((lax.axis_index("zh") * 4 + lax.axis_index("zl")) * 4 + lax.axis_index("y")) * ROWS
    pool_ref[0:16] = jnp.zeros((16, LANES), bf16)
    pool_ref[16:] = pool_rows(
        pool, pool[16:], place + 16, matrix_ref[0], lines_ref[6:7]
    ).astype(bf16)
    values_b = main_ref[:, 256:384]
    row = iota((ROWS, LANES), 0)
    col = iota((ROWS, LANES), 1)
    lane_low = col < HEAD
    upto = ((row // CHUNK) == (col // CHUNK)) & (row >= col)
    heads = (row // HEAD) == (col // HEAD)
    ones = jnp.where(heads, 1.0, 0.0).astype(bf16)
    out_ref[1] = mm_exact_right(wide_ref[1] * lines_ref[7:8], ones) * values_b.astype(f32)
    out_ref[2] = jnp.dot(low_ref[1], gw_ref[...], preferred_element_type=f32)
    scores = mm(
        jnp.concatenate(masked(hats_ref[0].astype(f32), lane_low), axis=0),
        jnp.concatenate([hats_ref[1], hats_ref[2]], axis=0),
        NT,
    )
    reads, direct = [], []
    for h in range(2):
        at = slice(h * ROWS, h * ROWS + ROWS)
        reads.append(mm(jnp.where(upto, scores[at, :ROWS], 0.0), solved_ref[h]))
        direct.append(mm(jnp.where(upto, scores[at, ROWS:], 0.0), values_b))
    y_local = jnp.where(lane_low, reads[0] + direct[0], reads[1] + direct[1])
    y_map = wide_ref[0] + pltpu.roll(jnp.where(lane_low, reads[1], reads[0]), HEAD, 1)
    first = first_ref[...].astype(f32)
    late = mm(
        y_map[CHUNK:],
        jnp.concatenate([block_diagonal(first[CHUNK:]), block_diagonal(first[:CHUNK])], axis=0),
        NT,
    )
    ymap_ref[:CHUNK] = y_map[:CHUNK].astype(bf16)
    ymap_ref[CHUNK:] = late[:, LANES:].astype(bf16)
    y_local = jnp.concatenate([y_local[:CHUNK], y_local[CHUNK:] + late[:, :LANES]], axis=0)
    mean = jnp.where(heads, 1.0 / HEAD, 0.0).astype(bf16)
    out_ref[0] = y_local - mm_exact_right(y_local, mean)


def identity_pair():
    eye = iota((HEAD, LANES), 0) == (iota((HEAD, LANES), 1) % HEAD)
    return jnp.concatenate([jnp.where(eye, 1.0, 0.0).astype(f32), jnp.zeros((HEAD, LANES), f32)], 0)


def compose(earlier, later):
    moved = mm(earlier, block_diagonal(later[:HEAD]))
    return jnp.concatenate([moved[:HEAD], moved[HEAD:] + later[HEAD:]], axis=0)


def chain(first, others):
    made = [first]
    for other in others:
        made.append(compose(made[-1], other))
    return made


def chosen_before(made, mine):
    before = jnp.where(mine == 0, identity_pair(), made[0])
    for j in (1, 2):
        before = jnp.where(mine > j, made[j], before)
    return before


def tail_before(got_ref, mine):
    found = jnp.zeros((16, LANES), f32)
    for j in range(3):
        found = jnp.where(mine == j + 1, got_ref[j, TAIL : TAIL + 16].astype(f32), found)
    return found


def prefixes(got_ref, mine):
    pieces = [got_ref[j, :128].astype(f32) for j in range(4)]
    made = chain(pieces[0], pieces[1:])
    return chosen_before(made, mine), made[3].astype(bf16)


def stage_y(got_ref, pay_ref, before_ref, tail_ref):
    y = lax.axis_index("y")
    before, running = prefixes(got_ref, y)
    before_ref[...] = before
    tail_ref[...] = tail_before(got_ref, y)
    extras = [got_ref[j, TAIL : TAIL + 16].astype(f32) for j in range(4)]
    line = extras[0] + extras[1] + extras[2] + extras[3]
    extra = jnp.where(iota((16, LANES), 0) == 0, line, extras[3]).astype(bf16)
    for j in range(4):
        pay_ref[j, 0:128] = running
        pay_ref[j, TAIL : TAIL + 16] = extra


def stage_zl(got_ref, before_ref, tail_ref, pay_ref, out_before_ref, out_tail_ref):
    y, zl = lax.axis_index("y"), lax.axis_index("zl")
    before, running = prefixes(got_ref, zl)
    out_before_ref[...] = compose(before, before_ref[...])
    out_tail_ref[...] = jnp.where(y == 0, tail_before(got_ref, zl), tail_ref[...])
    row = iota((16, LANES), 0)
    left = jnp.zeros((16, LANES), f32)
    for j in range(4):
        left = jnp.where(row == j, got_ref[j, TAIL : TAIL + 16].astype(f32)[0:1], left)
    pay_ref[0:128] = running
    pay_ref[TAIL : TAIL + 16] = got_ref[3, TAIL : TAIL + 16]
    pay_ref[LEFT : LEFT + 16] = left.astype(bf16)


def finish(
    got_ref, before_ref, tail_ref, start_ref, ymap_ref, yloc_ref, lines_ref,
    main_ref, pool_ref, matrix_ref, wout_ref, out_ref,
):
    zh, zl, y = lax.axis_index("zh"), lax.axis_index("zl"), lax.axis_index("y")
    state = jnp.concatenate([start_ref[0], start_ref[1]], axis=1)
    pieces = [got_ref[j, :128].astype(f32) for j in range(3)]
    advance = lambda old, piece: mm(old, block_diagonal(piece[:HEAD])) + piece[HEAD:]
    both = compose(pieces[1], pieces[2])
    state = jnp.where(zh > 0, advance(state, pieces[0]), state)
    after = jnp.where(zh > 2, both, pieces[1])
    state = jnp.where(zh > 1, advance(state, after), state)
    state = advance(state, before_ref[...])
    state = state - jnp.mean(state, axis=0, keepdims=True)
    off = yloc_ref[0] + mm(ymap_ref[...], block_diagonal(state), NT)
    row = iota((ROWS, LANES), 0)
    col = iota((ROWS, LANES), 1)
    mean = jnp.where((row // HEAD) == (col // HEAD), 1.0 / HEAD, 0.0).astype(bf16)
    spread = mm_exact_right(off * off, mean)
    headed = off * lax.rsqrt(spread + 1e-05 * HEAD) * lines_ref[4:5] + lines_ref[5:6] + yloc_ref[1]
    attn = (headed * yloc_ref[2]).astype(bf16)

    tail = jnp.where((y == 0) & (zl == 0), tail_before(got_ref, zh), tail_ref[...])
    head = main_ref[0:16, 384:512].astype(f32)
    place = ((zh * 4 + zl) * 4 + y) * ROWS
    opening = pool_rows(
        jnp.concatenate([tail, head], axis=0), head, place, matrix_ref[0], lines_ref[6:7]
    ).astype(bf16)
    pool_out = jnp.concatenate([opening, pool_ref[16:]], axis=0)

    acts = jnp.concatenate([attn, pool_out], axis=1)
    last = pool_out[:, 127:128].astype(f32)
    for zpair in range(8):
        rows = []
        for z in (2 * zpair, 2 * zpair + 1):
            for yy in range(4):
                rows.append(wout_ref[yy, 32 * z : 32 * z + 32])
        made = mm(acts, jnp.concatenate(rows, axis=0), NT)
        for half in range(2):
            z = 2 * zpair + half
            line = got_ref[z // 4, LEFT : LEFT + 16].astype(f32)[z % 4 : z % 4 + 1]
            out_ref[:, 128 * z : 128 * z + 128] = (
                made[:, 128 * half : 128 * half + 128] + last * line
            ).astype(bf16)


def add_parts(part_ref, out_ref):
    total = part_ref[0].astype(f32)
    for j in range(1, 8):
        total = total + part_ref[j].astype(f32)
    out_ref[...] = total.astype(bf16)


def on_device(
    tokens, input_norm_scale, input_norm_bias, query_projection, key_projection,
    value_projection, pooling_input_projection, decay_input_weight, rate_input_weight,
    gate_input_weight, decay_output_weight, rate_output_weight, gate_output_weight,
    decay_bias_base, learning_rate_base, key_prenorm_scale, key_learning_scale,
    self_term_weight, head_norm_scale, head_norm_bias, rate_extra_log, decay_extra_log,
    starting_head_state, pooling_group_matrix, pooling_output_scale, output_attention_rows,
    output_pooling_rows,
):
    line = lambda v: v.reshape(1, -1)
    sent, lines = call(
        prepare_tokens, [shaped((4, 128, 512), bf16), shaped((8, 128), f32)],
        tokens, line(input_norm_scale), line(input_norm_bias), line(decay_bias_base),
        line(learning_rate_base), line(key_prenorm_scale), line(key_learning_scale),
        line(head_norm_scale), line(head_norm_bias), line(pooling_output_scale),
        line(self_term_weight), name="prepare_tokens",
        space=pltpu.HBM, vmem=60 * 2**20,
        scratch=[
            pltpu.VMEM((128, 2048), bf16), pltpu.VMEM((1, 2048), f32), pltpu.VMEM((1, 2048), f32),
            pltpu.SemaphoreType.DMA((11,)),
        ],
    )
    shard, left = call(
        prepare_weights, [shaped((32, 1023), bf16), shaped((16, 128), f32)],
        query_projection, key_projection, value_projection, pooling_input_projection,
        decay_input_weight, rate_input_weight, gate_input_weight, output_attention_rows.T,
        output_pooling_rows.T, name="prepare_weights",
    )
    gathered = lax.all_gather(shard, Z, axis=0, tiled=True)
    mixed_tokens = lax.all_to_all(sent, "y", 0, 0, tiled=True).reshape(512, 512)
    parts = call(
        partial_products, shaped((4, 128, 768), bf16), mixed_tokens, gathered,
        name="partial_products",
    )
    parts = lax.all_to_all(parts, "y", 0, 0, tiled=True)
    main, low = call(
        sum_parts, [shaped((128, 512), bf16), shaped((128, 256), bf16)], parts, name="sum_parts"
    )
    low = lax.all_gather(low, "c", axis=0)
    pay, solved, hats, first, wide = call(
        block_maps,
        [
            shaped((4, PAY, 128), bf16), shaped((2, 128, 128), bf16), shaped((3, 128, 128), bf16),
            shaped((128, 128), bf16), shaped((2, 128, 128), f32),
        ],
        main, low, decay_output_weight, rate_output_weight, lines, rate_extra_log,
        decay_extra_log, left, name="block_maps",
    )
    columns, pay = lax.optimization_barrier((gathered, pay))
    got = lax.all_to_all(pay, "y", 0, 0, tiled=True)
    columns = call(spread_columns, shaped((4, 512, 256), bf16), columns, name="spread_columns")
    y_map, y_local, pool_out = call(
        block_readings,
        [shaped((128, 128), bf16), shaped((3, 128, 128), f32), shaped((128, 128), bf16)],
        main, low, gate_output_weight, solved, hats, first, wide, lines, pooling_group_matrix,
        name="block_readings",
    )
    pay, before, tail = call(
        stage_y,
        [shaped((4, PAY, 128), bf16), shaped((128, 128), f32), shaped((16, 128), f32)],
        got, name="stage_y",
    )
    got = lax.all_to_all(pay, "zl", 0, 0, tiled=True)
    columns, got, y_map = lax.optimization_barrier((columns, got, y_map))
    columns = lax.all_to_all(columns, "y", 0, 0, tiled=True)
    pay, before, tail = call(
        stage_zl,
        [shaped((WIDE, 128), bf16), shaped((128, 128), f32), shaped((16, 128), f32)],
        got, before, tail, name="stage_zl",
    )
    got = lax.all_gather(pay, "zh", axis=0)
    out = call(
        finish, shaped((128, 2048), bf16),
        got, before, tail, starting_head_state, y_map, y_local, lines, main, pool_out,
        pooling_group_matrix, columns, name="finish",
    )
    parts = lax.all_to_all(out.reshape(8, 16, 2048), TP, 0, 0, tiled=True)
    return call(add_parts, shaped((16, 2048), bf16), parts, name="add_parts")


def solution(mesh):
    split = Mesh(mesh.devices.reshape(4, 4, 4, 4, 2), ("zh", "zl", "y", "x", "c"))
    in_specs = (
        P(SP, None), P(), P(),
        P(SP, TP), P(SP, TP), P(SP, TP), P(SP, TP),
        P(SP, None), P(SP, None), P(SP, None),
        P(None, TP), P(None, TP), P(None, TP),
        P(TP), P(TP), P(TP), P(TP), P(TP), P(TP), P(TP),
        P(SP, TP), P(SP, TP),
        P(TP, None, None), P(TP, None, None), P(TP),
        P(TP, SP), P(TP, SP),
    )
    out_specs = P((*SP, *TP), None)
    return jax.shard_map(
        on_device, mesh=split, in_specs=in_specs, out_specs=out_specs, check_vma=False
    )
```

```python
import functools

import jax
import jax.numpy as jnp
from jax import lax
from jax.experimental import pallas as pl
from jax.experimental.pallas import tpu as pltpu
from jax.sharding import Mesh
from jax.sharding import PartitionSpec as P

Z = ("zh", "zl")
SP = ("zh", "zl", "y")
TP = ("x", "c")
f32 = jnp.float32
bf16 = jnp.bfloat16
HEAD = 64
CHUNK = 64
ROWS = 128
LANES = 128
PAY = 144
WIDE = 160
TAIL = 128
LEFT = 144
NT = (((1,), (1,)), ((), ()))
TN = (((0,), (0,)), ((), ()))


def iota(shape, dim):
    return lax.broadcasted_iota(jnp.int32, shape, dim)


def mm(a, b, dims=(((1,), (0,)), ((), ()))):
    return lax.dot_general(a.astype(bf16), b.astype(bf16), dims, preferred_element_type=f32)


def split(x, parts):
    found = []
    for _ in range(parts):
        piece = x.astype(bf16)
        found.append(piece)
        x = x - piece.astype(f32)
    return found


def mm_exact_right(x, exact):
    return jnp.dot(
        jnp.concatenate(split(x, 3), axis=1),
        jnp.concatenate([exact] * 3, axis=0),
        preferred_element_type=f32,
    )


def mm_exact_left(exact, x):
    return jnp.dot(
        jnp.concatenate([exact] * 3, axis=1),
        jnp.concatenate(split(x, 3), axis=0),
        preferred_element_type=f32,
    )


def mm_wide(a, b):
    a0, a1 = split(a, 2)
    b0, b1 = split(b, 2)
    return jnp.dot(
        jnp.concatenate([a0, a0, a1], axis=1),
        jnp.concatenate([b0, b1, b0], axis=0),
        preferred_element_type=f32,
    )


def call(kernel, outs, *args, flops=10**8, name=None, vmem=16 * 2**20, space=pltpu.VMEM, scratch=()):
    size = sum(a.size * a.dtype.itemsize for a in args)
    return pl.pallas_call(
        kernel,
        out_shape=outs,
        in_specs=[pl.BlockSpec(memory_space=space)] * len(args),
        out_specs=jax.tree.map(lambda _: pl.BlockSpec(memory_space=pltpu.VMEM), outs),
        scratch_shapes=scratch,
        compiler_params=pltpu.CompilerParams(vmem_limit_bytes=vmem),
        cost_estimate=pl.CostEstimate(flops=flops, bytes_accessed=size, transcendentals=0),
        name=name,
    )(*args)


def shaped(shape, dtype):
    return jax.ShapeDtypeStruct(shape, dtype)


def prepare_tokens(tok_hbm, gain_hbm, bias_hbm, *rest):
    *vectors, out_ref, lines_ref, tok, gain, bias, sems = rest
    lines = [
        pltpu.make_async_copy(ref, lines_ref.at[pl.ds(i, 1)], sems.at[3 + i])
        for i, ref in enumerate(vectors)
    ]
    copies = [
        pltpu.make_async_copy(tok_hbm, tok, sems.at[0]),
        pltpu.make_async_copy(gain_hbm, gain, sems.at[1]),
        pltpu.make_async_copy(bias_hbm, bias, sems.at[2]),
        *lines,
    ]
    for copy in copies:
        copy.start()
    source = iota((512, 512), 0)
    target = iota((512, 512), 1)
    moved = ((source >> 5) & 3) * 128 + (source >> 7) * 32 + (source & 31)
    pick = jnp.where(moved == target, 1.0, 0.0).astype(bf16)
    for copy in copies:
        copy.wait()
    wide = tok[...].astype(f32)
    center = jnp.mean(wide, axis=-1, keepdims=True)
    off = wide - center
    spread = jnp.mean(jnp.square(off), axis=-1, keepdims=True)
    normed = (off * lax.rsqrt(spread + 1e-05) * gain[...] + bias[...]).astype(bf16)
    for j in range(4):
        turned = jnp.dot(normed[:, 512 * j : 512 * j + 512], pick, preferred_element_type=f32)
        for y in range(4):
            out_ref[y, :, 128 * j : 128 * j + 128] = turned[:, 128 * y : 128 * y + 128].astype(bf16)


def prepare_weights(
    q_ref, k_ref, v_ref, p_ref, d_ref, r_ref, g_ref, oa_ref, op_ref, out_ref, left_ref
):
    first = lax.axis_index("c") == 0
    out_ref[:, 0:128] = q_ref[...]
    out_ref[:, 128:256] = k_ref[...]
    out_ref[:, 256:384] = v_ref[...]
    out_ref[:, 384:512] = p_ref[...]
    gate = g_ref[...]
    out_ref[:, 512:640] = jnp.where(first, d_ref[...], gate[:, :128])
    out_ref[:, 640:768] = jnp.where(first, r_ref[...], gate[:, 128:])
    out_ref[:, 768:896] = oa_ref[...]
    out_ref[:, 896:1023] = op_ref[:, :127]
    spot = iota((32, LANES), 1) == lax.axis_index("y") * 32 + iota((32, LANES), 0)
    column = op_ref[...].astype(f32)[:, 127:128]
    line = jnp.sum(jnp.where(spot, column, 0.0), axis=0, keepdims=True)
    left_ref[...] = jnp.where(iota((16, LANES), 0) == 0, line, 0.0)


def partial_products(tok_ref, w_ref, lines_ref, part_ref, out_lines_ref):
    out_lines_ref[...] = lines_ref[...]
    made = jnp.dot(tok_ref[...], w_ref[:, :768], preferred_element_type=f32).astype(bf16)
    for y in range(4):
        part_ref[y] = made[128 * y : 128 * y + 128]


def spread_columns(w_ref, out_ref):
    first = w_ref[:, 768:896]
    second = w_ref[:, 896:1023]
    for y in range(4):
        out_ref[y, :, 0:128] = first
        out_ref[y, :, 128:255] = second
        out_ref[y, :, 255:256] = jnp.zeros((512, 1), bf16)


def sum_parts(part_ref, main_ref, low_ref):
    total = part_ref[0].astype(f32)
    for y in range(1, 4):
        total = total + part_ref[y].astype(f32)
    rounded = total.astype(bf16)
    main_ref[...] = rounded[:, :512]
    low = rounded[:, 512:].astype(f32)
    first = lax.axis_index("c") == 0
    one = jnp.where(first, jnp.tanh(low[:, :128]), jax.nn.sigmoid(low[:, :128]))
    two = jnp.where(first, low[:, 128:], jax.nn.sigmoid(low[:, 128:]))
    low_ref[:, :128] = one.astype(bf16)
    low_ref[:, 128:] = two.astype(bf16)


def masked(x, lane_low):
    zero = jnp.zeros_like(x)
    return [jnp.where(lane_low, x, zero), jnp.where(lane_low, zero, x)]


def block_diagonal(pair):
    low = iota(pair.shape, 1) < HEAD
    zero = jnp.zeros_like(pair)
    return jnp.concatenate([jnp.where(low, pair, zero), jnp.where(low, zero, pair)], axis=0)


def block_maps(
    main_ref, low_ref, dw_ref, rw_ref, lines_ref, re_ref, de_ref, left_ref, pay_ref, solved_ref, hats_ref, first_ref, wide_ref,
):
    line = lambda i: lines_ref[i : i + 1]
    recept = main_ref[:, 0:128].astype(f32)
    keys = main_ref[:, 128:256].astype(f32)
    values_b = main_ref[:, 256:384]
    row = iota((ROWS, LANES), 0)
    col = iota((ROWS, LANES), 1)
    lane_low = col < HEAD
    same = (row // CHUNK) == (col // CHUNK)

    drive = line(0) + jnp.dot(low_ref[0, :, :128], dw_ref[...], preferred_element_type=f32)
    log_decay = -jax.nn.sigmoid(drive) * jnp.exp(re_ref[...] - 0.5) + de_ref[...]
    rate = jax.nn.sigmoid(
        line(1) + jnp.dot(low_ref[0, :, 128:], rw_ref[...], preferred_element_type=f32)
    )

    ones = jnp.where(same, 1.0, 0.0).astype(bf16)
    unit = keys * line(2)
    effective = keys * (1.0 + (rate - 1.0) * line(3))
    unit = unit * lax.rsqrt(mm_exact_right(unit * unit, ones) + 1e-06)
    wide_ref[1] = recept * effective
    beta = unit * rate

    tril = jnp.where(same & (row >= col), 1.0, 0.0).astype(bf16)
    totals = mm_exact_left(jnp.concatenate([tril, ones], axis=0), log_decay)
    total, end = totals[:ROWS], totals[ROWS:]
    ref = 0.5 * end
    grow = jnp.exp(ref - total)
    shrink = jnp.exp(total - ref)
    base = jnp.exp(ref)
    a_hat = -unit * jnp.exp(total - log_decay - ref)
    r_hat = recept * shrink
    b_hat = beta * grow
    k_hat = effective * grow
    wide_ref[0] = r_hat * base
    hats_ref[0] = r_hat.astype(bf16)
    hats_ref[1] = b_hat.astype(bf16)
    hats_ref[2] = k_hat.astype(bf16)

    left = jnp.concatenate(masked(a_hat, lane_low), axis=0)
    right = jnp.concatenate([b_hat, k_hat], axis=0)
    scores = mm(left, right, NT)
    strict = same & (row > col)
    eye = jnp.where(row == col, 1.0, 0.0).astype(f32)
    swapped = pltpu.roll(a_hat * base, HEAD, 1)
    full = [jnp.where(strict, scores[h * ROWS : h * ROWS + ROWS, :ROWS], 0.0) for h in range(2)]
    within = {n: (row // n) == (col // n) for n in (8, 16, 32)}
    power = [jnp.where(within[8], full[h], 0.0) for h in range(2)]
    product = [eye + power[h] for h in range(2)]
    for _ in range(2):
        power = [mm_wide(power[h], power[h]) for h in range(2)]
        product = [product[h] + mm_wide(product[h], power[h]) for h in range(2)]
    for here in (within[16] & ~within[8], within[32] & ~within[16], ~within[32]):
        mid = [mm_wide(product[h], jnp.where(here, full[h], 0.0)) for h in range(2)]
        product = [product[h] + mm_wide(mid[h], product[h]) for h in range(2)]
    solved = []
    for h in range(2):
        pushed = mm(jnp.where(strict, scores[h * ROWS : h * ROWS + ROWS, ROWS:], 0.0), values_b)
        rhs = jnp.where(lane_low if h == 0 else ~lane_low, pushed, swapped)
        solved.append(mm(product[h], rhs).astype(bf16))
        solved_ref[h] = solved[h]

    b_end = (b_hat * base).astype(bf16)
    k_end = (k_hat * base).astype(bf16)
    decay_end = jnp.exp(end)
    low64 = iota((CHUNK, LANES), 1) < HEAD
    diagonal = iota((CHUNK, LANES), 0) == (iota((CHUNK, LANES), 1) % HEAD)
    maps, states = [], []
    for c in range(2):
        at = slice(c * CHUNK, c * CHUNK + CHUNK)
        g0 = mm(solved[0][at], b_end[at], TN)
        g1 = mm(solved[1][at], b_end[at], TN)
        kv = mm(values_b[at], k_end[at], TN)
        maps.append(
            jnp.where(diagonal, decay_end[at], 0.0) + jnp.where(low64, g0[HEAD:], g1[:HEAD])
        )
        states.append(
            jnp.where(low64, g0[:HEAD], g1[HEAD:]) + jnp.where(low64, kv[:HEAD], kv[HEAD:])
        )
    chunk0 = jnp.concatenate([maps[0], states[0]], axis=0).astype(bf16)
    first_ref[...] = chunk0
    joined = mm(chunk0, block_diagonal(maps[1]))
    block_map = joined[:CHUNK].astype(bf16)
    block_state = (joined[CHUNK:] + states[1]).astype(bf16)
    tail = main_ref[ROWS - 16 :, 384:512].astype(f32)
    extra = jnp.where(row[:16] == 0, left_ref[...], tail).astype(bf16)
    for j in range(4):
        pay_ref[j, 0:64] = block_map
        pay_ref[j, 64:128] = block_state
        pay_ref[j, TAIL : TAIL + 16] = extra


def pool_rows(extended, own, place, matrix, scale):
    level = lax.axis_index("x")
    sums = extended
    chosen = None
    for k in range(4):
        width = 1 << k
        sums = sums + pltpu.roll(sums, width, 0)
        picked = sums[16:]
        chosen = picked if k == 0 else jnp.where(level >= k, picked, chosen)
    window = lax.shift_left(jnp.int32(2), level).astype(f32)
    position = (place + iota(own.shape, 0)).astype(f32)
    pooled = (chosen / jnp.minimum(position + 1.0, window) - own).astype(bf16)
    return jnp.dot(pooled, matrix, preferred_element_type=f32) * scale


def block_readings(
    main_ref, low_ref, gw_ref, solved_ref, hats_ref, first_ref, wide_ref, lines_ref, matrix_ref,
    ymap_ref, out_ref, pool_ref,
):
    pool = main_ref[:, 384:512].astype(f32)
    place = ((lax.axis_index("zh") * 4 + lax.axis_index("zl")) * 4 + lax.axis_index("y")) * ROWS
    pool_ref[0:16] = jnp.zeros((16, LANES), bf16)
    pool_ref[16:] = pool_rows(
        pool, pool[16:], place + 16, matrix_ref[0], lines_ref[6:7]
    ).astype(bf16)
    values_b = main_ref[:, 256:384]
    row = iota((ROWS, LANES), 0)
    col = iota((ROWS, LANES), 1)
    lane_low = col < HEAD
    upto = ((row // CHUNK) == (col // CHUNK)) & (row >= col)
    heads = (row // HEAD) == (col // HEAD)
    ones = jnp.where(heads, 1.0, 0.0).astype(bf16)
    out_ref[1] = mm_exact_right(wide_ref[1] * lines_ref[7:8], ones) * values_b.astype(f32)
    out_ref[2] = jnp.dot(low_ref[1], gw_ref[...], preferred_element_type=f32)
    scores = mm(
        jnp.concatenate(masked(hats_ref[0].astype(f32), lane_low), axis=0),
        jnp.concatenate([hats_ref[1], hats_ref[2]], axis=0),
        NT,
    )
    reads, direct = [], []
    for h in range(2):
        at = slice(h * ROWS, h * ROWS + ROWS)
        reads.append(mm(jnp.where(upto, scores[at, :ROWS], 0.0), solved_ref[h]))
        direct.append(mm(jnp.where(upto, scores[at, ROWS:], 0.0), values_b))
    y_local = jnp.where(lane_low, reads[0] + direct[0], reads[1] + direct[1])
    y_map = wide_ref[0] + pltpu.roll(jnp.where(lane_low, reads[1], reads[0]), HEAD, 1)
    first = first_ref[...].astype(f32)
    late = mm(
        y_map[CHUNK:],
        jnp.concatenate([block_diagonal(first[CHUNK:]), block_diagonal(first[:CHUNK])], axis=0),
        NT,
    )
    ymap_ref[:CHUNK] = y_map[:CHUNK].astype(bf16)
    ymap_ref[CHUNK:] = late[:, LANES:].astype(bf16)
    y_local = jnp.concatenate([y_local[:CHUNK], y_local[CHUNK:] + late[:, :LANES]], axis=0)
    mean = jnp.where(heads, 1.0 / HEAD, 0.0).astype(bf16)
    out_ref[0] = y_local - mm_exact_right(y_local, mean)


def identity_pair():
    eye = iota((HEAD, LANES), 0) == (iota((HEAD, LANES), 1) % HEAD)
    return jnp.concatenate([jnp.where(eye, 1.0, 0.0).astype(f32), jnp.zeros((HEAD, LANES), f32)], 0)


def compose(earlier, later):
    moved = mm(earlier, block_diagonal(later[:HEAD]))
    return jnp.concatenate([moved[:HEAD], moved[HEAD:] + later[HEAD:]], axis=0)


def tail_before(got_ref, mine):
    found = jnp.zeros((16, LANES), f32)
    for j in range(3):
        found = jnp.where(mine == j + 1, got_ref[j, TAIL : TAIL + 16].astype(f32), found)
    return found


def prefixes(got_ref, mine):
    pieces = [got_ref[j, :128].astype(f32) for j in range(4)]
    two = compose(pieces[0], pieces[1])
    three = compose(two, pieces[2])
    whole = compose(two, compose(pieces[2], pieces[3]))
    before = jnp.where(mine == 0, identity_pair(), pieces[0])
    before = jnp.where(mine > 1, two, before)
    before = jnp.where(mine > 2, three, before)
    return before, whole.astype(bf16)


def stage_y(got_ref, pay_ref, before_ref, tail_ref):
    y = lax.axis_index("y")
    before, running = prefixes(got_ref, y)
    before_ref[...] = before
    tail_ref[...] = tail_before(got_ref, y)
    extras = [got_ref[j, TAIL : TAIL + 16].astype(f32) for j in range(4)]
    line = extras[0] + extras[1] + extras[2] + extras[3]
    extra = jnp.where(iota((16, LANES), 0) == 0, line, extras[3]).astype(bf16)
    for j in range(4):
        pay_ref[j, 0:128] = running
        pay_ref[j, TAIL : TAIL + 16] = extra


def stage_zl(got_ref, before_ref, tail_ref, pay_ref, out_before_ref, out_tail_ref):
    y, zl = lax.axis_index("y"), lax.axis_index("zl")
    before, running = prefixes(got_ref, zl)
    out_before_ref[...] = compose(before, before_ref[...])
    out_tail_ref[...] = jnp.where(y == 0, tail_before(got_ref, zl), tail_ref[...])
    row = iota((16, LANES), 0)
    left = jnp.zeros((16, LANES), f32)
    for j in range(4):
        left = jnp.where(row == j, got_ref[j, TAIL : TAIL + 16].astype(f32)[0:1], left)
    pay_ref[0:128] = running
    pay_ref[TAIL : TAIL + 16] = got_ref[3, TAIL : TAIL + 16]
    pay_ref[LEFT : LEFT + 16] = left.astype(bf16)


def finish(
    got_ref, before_ref, tail_ref, start_ref, ymap_ref, yloc_ref, lines_ref,
    main_ref, pool_ref, matrix_ref, wout_ref, out_ref,
):
    zh, zl, y = lax.axis_index("zh"), lax.axis_index("zl"), lax.axis_index("y")
    state = jnp.concatenate([start_ref[0], start_ref[1]], axis=1)
    pieces = [got_ref[j, :128].astype(f32) for j in range(3)]
    advance = lambda old, piece: mm(old, block_diagonal(piece[:HEAD])) + piece[HEAD:]
    both = compose(pieces[1], pieces[2])
    state = jnp.where(zh > 0, advance(state, pieces[0]), state)
    after = jnp.where(zh > 2, both, pieces[1])
    state = jnp.where(zh > 1, advance(state, after), state)
    state = advance(state, before_ref[...])
    state = state - jnp.mean(state, axis=0, keepdims=True)
    off = yloc_ref[0] + mm(ymap_ref[...], block_diagonal(state), NT)
    row = iota((ROWS, LANES), 0)
    col = iota((ROWS, LANES), 1)
    mean = jnp.where((row // HEAD) == (col // HEAD), 1.0 / HEAD, 0.0).astype(bf16)
    spread = mm_exact_right(off * off, mean)
    headed = off * lax.rsqrt(spread + 1e-05 * HEAD) * lines_ref[4:5] + lines_ref[5:6] + yloc_ref[1]
    attn = (headed * yloc_ref[2]).astype(bf16)

    tail = jnp.where((y == 0) & (zl == 0), tail_before(got_ref, zh), tail_ref[...])
    head = main_ref[0:16, 384:512].astype(f32)
    place = ((zh * 4 + zl) * 4 + y) * ROWS
    opening = pool_rows(
        jnp.concatenate([tail, head], axis=0), head, place, matrix_ref[0], lines_ref[6:7]
    ).astype(bf16)
    pool_out = jnp.concatenate([opening, pool_ref[16:]], axis=0)

    acts = jnp.concatenate([attn, pool_out], axis=1)
    last = pool_out[:, 127:128].astype(f32)
    for zpair in range(8):
        rows = []
        for z in (2 * zpair, 2 * zpair + 1):
            for yy in range(4):
                rows.append(wout_ref[yy, 32 * z : 32 * z + 32])
        made = mm(acts, jnp.concatenate(rows, axis=0), NT)
        for half in range(2):
            z = 2 * zpair + half
            line = got_ref[z // 4, LEFT : LEFT + 16].astype(f32)[z % 4 : z % 4 + 1]
            out_ref[:, 128 * z : 128 * z + 128] = (
                made[:, 128 * half : 128 * half + 128] + last * line
            ).astype(bf16)


def add_parts(part_ref, out_ref):
    total = part_ref[0].astype(f32)
    for j in range(1, 8):
        total = total + part_ref[j].astype(f32)
    out_ref[...] = total.astype(bf16)


def on_device(
    tokens, input_norm_scale, input_norm_bias, query_projection, key_projection,
    value_projection, pooling_input_projection, decay_input_weight, rate_input_weight,
    gate_input_weight, decay_output_weight, rate_output_weight, gate_output_weight,
    decay_bias_base, learning_rate_base, key_prenorm_scale, key_learning_scale,
    self_term_weight, head_norm_scale, head_norm_bias, rate_extra_log, decay_extra_log,
    starting_head_state, pooling_group_matrix, pooling_output_scale, output_attention_rows,
    output_pooling_rows,
):
    line = lambda v: v.reshape(1, -1)
    sent, lines = call(
        prepare_tokens, [shaped((4, 128, 512), bf16), shaped((8, 128), f32)],
        tokens, line(input_norm_scale), line(input_norm_bias), line(decay_bias_base),
        line(learning_rate_base), line(key_prenorm_scale), line(key_learning_scale),
        line(head_norm_scale), line(head_norm_bias), line(pooling_output_scale),
        line(self_term_weight), name="prepare_tokens",
        space=pltpu.HBM, vmem=60 * 2**20,
        scratch=[
            pltpu.VMEM((128, 2048), bf16), pltpu.VMEM((1, 2048), f32), pltpu.VMEM((1, 2048), f32),
            pltpu.SemaphoreType.DMA((11,)),
        ],
    )
    shard, left = call(
        prepare_weights, [shaped((32, 1023), bf16), shaped((16, 128), f32)],
        query_projection, key_projection, value_projection, pooling_input_projection,
        decay_input_weight, rate_input_weight, gate_input_weight, output_attention_rows.T,
        output_pooling_rows.T, name="prepare_weights",
    )
    gathered = lax.all_gather(shard, Z, axis=0, tiled=True)
    mixed_tokens = lax.all_to_all(sent, "y", 0, 0, tiled=True).reshape(512, 512)
    parts, lines = call(
        partial_products, [shaped((4, 128, 768), bf16), shaped((8, 128), f32)],
        mixed_tokens, gathered, lines, name="partial_products",
    )
    parts = lax.all_to_all(parts, "y", 0, 0, tiled=True)
    main, low = call(
        sum_parts, [shaped((128, 512), bf16), shaped((128, 256), bf16)], parts, name="sum_parts"
    )
    low = lax.all_gather(low, "c", axis=0)
    pay, solved, hats, first, wide = call(
        block_maps,
        [
            shaped((4, PAY, 128), bf16), shaped((2, 128, 128), bf16), shaped((3, 128, 128), bf16),
            shaped((128, 128), bf16), shaped((2, 128, 128), f32),
        ],
        main, low, decay_output_weight, rate_output_weight, lines, rate_extra_log,
        decay_extra_log, left, name="block_maps",
    )
    columns, pay = lax.optimization_barrier((gathered, pay))
    got = lax.all_to_all(pay, "y", 0, 0, tiled=True)
    columns = call(spread_columns, shaped((4, 512, 256), bf16), columns, name="spread_columns")
    y_map, y_local, pool_out = call(
        block_readings,
        [shaped((128, 128), bf16), shaped((3, 128, 128), f32), shaped((128, 128), bf16)],
        main, low, gate_output_weight, solved, hats, first, wide, lines, pooling_group_matrix,
        name="block_readings",
    )
    pay, before, tail = call(
        stage_y,
        [shaped((4, PAY, 128), bf16), shaped((128, 128), f32), shaped((16, 128), f32)],
        got, name="stage_y",
    )
    got = lax.all_to_all(pay, "zl", 0, 0, tiled=True)
    columns, got, y_map = lax.optimization_barrier((columns, got, y_map))
    columns = lax.all_to_all(columns, "y", 0, 0, tiled=True)
    pay, before, tail = call(
        stage_zl,
        [shaped((WIDE, 128), bf16), shaped((128, 128), f32), shaped((16, 128), f32)],
        got, before, tail, name="stage_zl",
    )
    got = lax.all_gather(pay, "zh", axis=0)
    out = call(
        finish, shaped((128, 2048), bf16),
        got, before, tail, starting_head_state, y_map, y_local, lines, main, pool_out,
        pooling_group_matrix, columns, name="finish",
    )
    parts = lax.all_to_all(out.reshape(8, 16, 2048), TP, 0, 0, tiled=True)
    return call(add_parts, shaped((16, 2048), bf16), parts, name="add_parts")


def solution(mesh):
    split = Mesh(mesh.devices.reshape(4, 4, 4, 4, 2), ("zh", "zl", "y", "x", "c"))
    in_specs = (
        P(SP, None), P(), P(),
        P(SP, TP), P(SP, TP), P(SP, TP), P(SP, TP),
        P(SP, None), P(SP, None), P(SP, None),
        P(None, TP), P(None, TP), P(None, TP),
        P(TP), P(TP), P(TP), P(TP), P(TP), P(TP), P(TP),
        P(SP, TP), P(SP, TP),
        P(TP, None, None), P(TP, None, None), P(TP),
        P(TP, SP), P(TP, SP),
    )
    out_specs = P((*SP, *TP), None)
    return jax.shard_map(
        on_device, mesh=split, in_specs=in_specs, out_specs=out_specs, check_vma=False
    )
```

```python
import functools

import jax
import jax.numpy as jnp
from jax import lax
from jax.experimental import pallas as pl
from jax.experimental.pallas import tpu as pltpu
from jax.sharding import Mesh
from jax.sharding import PartitionSpec as P

Z = ("zh", "zl")
SP = ("zh", "zl", "y")
TP = ("x", "c")
f32 = jnp.float32
bf16 = jnp.bfloat16
HEAD = 64
CHUNK = 64
ROWS = 128
LANES = 128
PAY = 144
WIDE = 160
TAIL = 128
LEFT = 144
NT = (((1,), (1,)), ((), ()))
TN = (((0,), (0,)), ((), ()))


def iota(shape, dim):
    return lax.broadcasted_iota(jnp.int32, shape, dim)


def mm(a, b, dims=(((1,), (0,)), ((), ()))):
    return lax.dot_general(a.astype(bf16), b.astype(bf16), dims, preferred_element_type=f32)


def split(x, parts):
    found = []
    for _ in range(parts):
        piece = x.astype(bf16)
        found.append(piece)
        x = x - piece.astype(f32)
    return found


def mm_exact_right(x, exact):
    return jnp.dot(
        jnp.concatenate(split(x, 3), axis=1),
        jnp.concatenate([exact] * 3, axis=0),
        preferred_element_type=f32,
    )


def mm_exact_left(exact, x):
    return jnp.dot(
        jnp.concatenate([exact] * 3, axis=1),
        jnp.concatenate(split(x, 3), axis=0),
        preferred_element_type=f32,
    )


def mm_wide(a, b):
    a0, a1 = split(a, 2)
    b0, b1 = split(b, 2)
    return jnp.dot(
        jnp.concatenate([a0, a0, a1], axis=1),
        jnp.concatenate([b0, b1, b0], axis=0),
        preferred_element_type=f32,
    )


def call(kernel, outs, *args, flops=10**8, name=None, vmem=16 * 2**20, space=pltpu.VMEM, scratch=(), places=None):
    size = sum(a.size * a.dtype.itemsize for a in args)
    return pl.pallas_call(
        kernel,
        out_shape=outs,
        in_specs=[pl.BlockSpec(memory_space=space)] * len(args),
        out_specs=places or jax.tree.map(lambda _: pl.BlockSpec(memory_space=pltpu.VMEM), outs),
        scratch_shapes=scratch,
        compiler_params=pltpu.CompilerParams(vmem_limit_bytes=vmem),
        cost_estimate=pl.CostEstimate(flops=flops, bytes_accessed=size, transcendentals=0),
        name=name,
    )(*args)


def shaped(shape, dtype):
    return jax.ShapeDtypeStruct(shape, dtype)


def prepare_tokens(tok_hbm, gain_hbm, bias_hbm, *rest):
    *vectors, out_ref, lines_ref, tok, gain, bias, sems = rest
    lines = [
        pltpu.make_async_copy(ref, lines_ref.at[pl.ds(i, 1)], sems.at[3 + i])
        for i, ref in enumerate(vectors)
    ]
    copies = [
        pltpu.make_async_copy(tok_hbm, tok, sems.at[0]),
        pltpu.make_async_copy(gain_hbm, gain, sems.at[1]),
        pltpu.make_async_copy(bias_hbm, bias, sems.at[2]),
        *lines,
    ]
    for copy in copies:
        copy.start()
    source = iota((512, 512), 0)
    target = iota((512, 512), 1)
    moved = ((source >> 5) & 3) * 128 + (source >> 7) * 32 + (source & 31)
    pick = jnp.where(moved == target, 1.0, 0.0).astype(bf16)
    for copy in copies:
        copy.wait()
    wide = tok[...].astype(f32)
    center = jnp.mean(wide, axis=-1, keepdims=True)
    off = wide - center
    spread = jnp.mean(jnp.square(off), axis=-1, keepdims=True)
    normed = (off * lax.rsqrt(spread + 1e-05) * gain[...] + bias[...]).astype(bf16)
    for j in range(4):
        turned = jnp.dot(normed[:, 512 * j : 512 * j + 512], pick, preferred_element_type=f32)
        for y in range(4):
            out_ref[y, :, 128 * j : 128 * j + 128] = turned[:, 128 * y : 128 * y + 128].astype(bf16)


def prepare_weights(
    q_ref, k_ref, v_ref, p_ref, d_ref, r_ref, g_ref, oa_ref, op_ref, out_ref, left_ref
):
    first = lax.axis_index("c") == 0
    out_ref[:, 0:128] = q_ref[...]
    out_ref[:, 128:256] = k_ref[...]
    out_ref[:, 256:384] = v_ref[...]
    out_ref[:, 384:512] = p_ref[...]
    gate = g_ref[...]
    out_ref[:, 512:640] = jnp.where(first, d_ref[...], gate[:, :128])
    out_ref[:, 640:768] = jnp.where(first, r_ref[...], gate[:, 128:])
    out_ref[:, 768:896] = oa_ref[...]
    out_ref[:, 896:1023] = op_ref[:, :127]
    spot = iota((32, LANES), 1) == lax.axis_index("y") * 32 + iota((32, LANES), 0)
    column = op_ref[...].astype(f32)[:, 127:128]
    line = jnp.sum(jnp.where(spot, column, 0.0), axis=0, keepdims=True)
    left_ref[...] = jnp.where(iota((16, LANES), 0) == 0, line, 0.0)


def partial_products(tok_ref, w_ref, lines_ref, part_ref, out_lines_ref, cols_ref):
    out_lines_ref[...] = lines_ref[...]
    cols_ref[:, 0:128] = w_ref[:, 768:896]
    cols_ref[:, 128:255] = w_ref[:, 896:1023]
    cols_ref[:, 255:256] = jnp.zeros((512, 1), bf16)
    made = jnp.dot(tok_ref[...], w_ref[:, :768], preferred_element_type=f32).astype(bf16)
    for y in range(4):
        part_ref[y] = made[128 * y : 128 * y + 128]


def sum_parts(part_ref, main_ref, low_ref):
    total = part_ref[0].astype(f32)
    for y in range(1, 4):
        total = total + part_ref[y].astype(f32)
    rounded = total.astype(bf16)
    main_ref[...] = rounded[:, :512]
    low = rounded[:, 512:].astype(f32)
    first = lax.axis_index("c") == 0
    one = jnp.where(first, jnp.tanh(low[:, :128]), jax.nn.sigmoid(low[:, :128]))
    two = jnp.where(first, low[:, 128:], jax.nn.sigmoid(low[:, 128:]))
    low_ref[:, :128] = one.astype(bf16)
    low_ref[:, 128:] = two.astype(bf16)


def masked(x, lane_low):
    zero = jnp.zeros_like(x)
    return [jnp.where(lane_low, x, zero), jnp.where(lane_low, zero, x)]


def block_diagonal(pair):
    low = iota(pair.shape, 1) < HEAD
    zero = jnp.zeros_like(pair)
    return jnp.concatenate([jnp.where(low, pair, zero), jnp.where(low, zero, pair)], axis=0)


def block_maps(
    main_ref, low_ref, dw_ref, rw_ref, lines_ref, re_ref, de_ref, left_ref, cols_ref,
    pay_ref, solved_ref, hats_ref, first_ref, wide_ref, spread_ref, sems,
):
    copies = [pltpu.make_async_copy(cols_ref, spread_ref.at[j], sems.at[j]) for j in range(4)]
    for copy in copies:
        copy.start()
    line = lambda i: lines_ref[i : i + 1]
    recept = main_ref[:, 0:128].astype(f32)
    keys = main_ref[:, 128:256].astype(f32)
    values_b = main_ref[:, 256:384]
    row = iota((ROWS, LANES), 0)
    col = iota((ROWS, LANES), 1)
    lane_low = col < HEAD
    same = (row // CHUNK) == (col // CHUNK)

    drive = line(0) + jnp.dot(low_ref[0, :, :128], dw_ref[...], preferred_element_type=f32)
    log_decay = -jax.nn.sigmoid(drive) * jnp.exp(re_ref[...] - 0.5) + de_ref[...]
    rate = jax.nn.sigmoid(
        line(1) + jnp.dot(low_ref[0, :, 128:], rw_ref[...], preferred_element_type=f32)
    )

    ones = jnp.where(same, 1.0, 0.0).astype(bf16)
    unit = keys * line(2)
    effective = keys * (1.0 + (rate - 1.0) * line(3))
    unit = unit * lax.rsqrt(mm_exact_right(unit * unit, ones) + 1e-06)
    wide_ref[1] = recept * effective
    beta = unit * rate

    tril = jnp.where(same & (row >= col), 1.0, 0.0).astype(bf16)
    totals = mm_exact_left(jnp.concatenate([tril, ones], axis=0), log_decay)
    total, end = totals[:ROWS], totals[ROWS:]
    ref = 0.5 * end
    grow = jnp.exp(ref - total)
    shrink = jnp.exp(total - ref)
    base = jnp.exp(ref)
    a_hat = -unit * jnp.exp(total - log_decay - ref)
    r_hat = recept * shrink
    b_hat = beta * grow
    k_hat = effective * grow
    wide_ref[0] = r_hat * base
    hats_ref[0] = r_hat.astype(bf16)
    hats_ref[1] = b_hat.astype(bf16)
    hats_ref[2] = k_hat.astype(bf16)

    left = jnp.concatenate(masked(a_hat, lane_low), axis=0)
    right = jnp.concatenate([b_hat, k_hat], axis=0)
    scores = mm(left, right, NT)
    strict = same & (row > col)
    eye = jnp.where(row == col, 1.0, 0.0).astype(f32)
    swapped = pltpu.roll(a_hat * base, HEAD, 1)
    full = [jnp.where(strict, scores[h * ROWS : h * ROWS + ROWS, :ROWS], 0.0) for h in range(2)]
    within = {n: (row // n) == (col // n) for n in (8, 16, 32)}
    power = [jnp.where(within[8], full[h], 0.0) for h in range(2)]
    product = [eye + power[h] for h in range(2)]
    for _ in range(2):
        power = [mm_wide(power[h], power[h]) for h in range(2)]
        product = [product[h] + mm_wide(product[h], power[h]) for h in range(2)]
    for here in (within[16] & ~within[8], within[32] & ~within[16], ~within[32]):
        mid = [mm_wide(product[h], jnp.where(here, full[h], 0.0)) for h in range(2)]
        product = [product[h] + mm_wide(mid[h], product[h]) for h in range(2)]
    solved = []
    for h in range(2):
        pushed = mm(jnp.where(strict, scores[h * ROWS : h * ROWS + ROWS, ROWS:], 0.0), values_b)
        rhs = jnp.where(lane_low if h == 0 else ~lane_low, pushed, swapped)
        solved.append(mm(product[h], rhs).astype(bf16))
        solved_ref[h] = solved[h]

    b_end = (b_hat * base).astype(bf16)
    k_end = (k_hat * base).astype(bf16)
    decay_end = jnp.exp(end)
    low64 = iota((CHUNK, LANES), 1) < HEAD
    diagonal = iota((CHUNK, LANES), 0) == (iota((CHUNK, LANES), 1) % HEAD)
    maps, states = [], []
    for c in range(2):
        at = slice(c * CHUNK, c * CHUNK + CHUNK)
        g0 = mm(solved[0][at], b_end[at], TN)
        g1 = mm(solved[1][at], b_end[at], TN)
        kv = mm(values_b[at], k_end[at], TN)
        maps.append(
            jnp.where(diagonal, decay_end[at], 0.0) + jnp.where(low64, g0[HEAD:], g1[:HEAD])
        )
        states.append(
            jnp.where(low64, g0[:HEAD], g1[HEAD:]) + jnp.where(low64, kv[:HEAD], kv[HEAD:])
        )
    chunk0 = jnp.concatenate([maps[0], states[0]], axis=0).astype(bf16)
    first_ref[...] = chunk0
    joined = mm(chunk0, block_diagonal(maps[1]))
    block_map = joined[:CHUNK].astype(bf16)
    block_state = (joined[CHUNK:] + states[1]).astype(bf16)
    tail = main_ref[ROWS - 16 :, 384:512].astype(f32)
    extra = jnp.where(row[:16] == 0, left_ref[...], tail).astype(bf16)
    for j in range(4):
        pay_ref[j, 0:64] = block_map
        pay_ref[j, 64:128] = block_state
        pay_ref[j, TAIL : TAIL + 16] = extra
    for copy in copies:
        copy.wait()


def pool_rows(extended, own, place, matrix, scale):
    level = lax.axis_index("x")
    sums = extended
    chosen = None
    for k in range(4):
        width = 1 << k
        sums = sums + pltpu.roll(sums, width, 0)
        picked = sums[16:]
        chosen = picked if k == 0 else jnp.where(level >= k, picked, chosen)
    window = lax.shift_left(jnp.int32(2), level).astype(f32)
    position = (place + iota(own.shape, 0)).astype(f32)
    pooled = (chosen / jnp.minimum(position + 1.0, window) - own).astype(bf16)
    return jnp.dot(pooled, matrix, preferred_element_type=f32) * scale


def block_readings(
    main_ref, low_ref, gw_ref, solved_ref, hats_ref, first_ref, wide_ref, lines_ref, matrix_ref,
    ymap_ref, out_ref, pool_ref,
):
    pool = main_ref[:, 384:512].astype(f32)
    place = ((lax.axis_index("zh") * 4 + lax.axis_index("zl")) * 4 + lax.axis_index("y")) * ROWS
    pool_ref[0:16] = jnp.zeros((16, LANES), bf16)
    pool_ref[16:] = pool_rows(
        pool, pool[16:], place + 16, matrix_ref[0], lines_ref[6:7]
    ).astype(bf16)
    values_b = main_ref[:, 256:384]
    row = iota((ROWS, LANES), 0)
    col = iota((ROWS, LANES), 1)
    lane_low = col < HEAD
    upto = ((row // CHUNK) == (col // CHUNK)) & (row >= col)
    heads = (row // HEAD) == (col // HEAD)
    ones = jnp.where(heads, 1.0, 0.0).astype(bf16)
    out_ref[1] = mm_exact_right(wide_ref[1] * lines_ref[7:8], ones) * values_b.astype(f32)
    out_ref[2] = jnp.dot(low_ref[1], gw_ref[...], preferred_element_type=f32)
    scores = mm(
        jnp.concatenate(masked(hats_ref[0].astype(f32), lane_low), axis=0),
        jnp.concatenate([hats_ref[1], hats_ref[2]], axis=0),
        NT,
    )
    reads, direct = [], []
    for h in range(2):
        at = slice(h * ROWS, h * ROWS + ROWS)
        reads.append(mm(jnp.where(upto, scores[at, :ROWS], 0.0), solved_ref[h]))
        direct.append(mm(jnp.where(upto, scores[at, ROWS:], 0.0), values_b))
    y_local = jnp.where(lane_low, reads[0] + direct[0], reads[1] + direct[1])
    y_map = wide_ref[0] + pltpu.roll(jnp.where(lane_low, reads[1], reads[0]), HEAD, 1)
    first = first_ref[...].astype(f32)
    late = mm(
        y_map[CHUNK:],
        jnp.concatenate([block_diagonal(first[CHUNK:]), block_diagonal(first[:CHUNK])], axis=0),
        NT,
    )
    ymap_ref[:CHUNK] = y_map[:CHUNK].astype(bf16)
    ymap_ref[CHUNK:] = late[:, LANES:].astype(bf16)
    y_local = jnp.concatenate([y_local[:CHUNK], y_local[CHUNK:] + late[:, :LANES]], axis=0)
    mean = jnp.where(heads, 1.0 / HEAD, 0.0).astype(bf16)
    out_ref[0] = y_local - mm_exact_right(y_local, mean)


def identity_pair():
    eye = iota((HEAD, LANES), 0) == (iota((HEAD, LANES), 1) % HEAD)
    return jnp.concatenate([jnp.where(eye, 1.0, 0.0).astype(f32), jnp.zeros((HEAD, LANES), f32)], 0)


def compose(earlier, later):
    moved = mm(earlier, block_diagonal(later[:HEAD]))
    return jnp.concatenate([moved[:HEAD], moved[HEAD:] + later[HEAD:]], axis=0)


def tail_before(got_ref, mine):
    found = jnp.zeros((16, LANES), f32)
    for j in range(3):
        found = jnp.where(mine == j + 1, got_ref[j, TAIL : TAIL + 16].astype(f32), found)
    return found


def prefixes(got_ref, mine):
    pieces = [got_ref[j, :128].astype(f32) for j in range(4)]
    two = compose(pieces[0], pieces[1])
    three = compose(two, pieces[2])
    whole = compose(two, compose(pieces[2], pieces[3]))
    before = jnp.where(mine == 0, identity_pair(), pieces[0])
    before = jnp.where(mine > 1, two, before)
    before = jnp.where(mine > 2, three, before)
    return before, whole.astype(bf16)


def stage_y(got_ref, pay_ref, before_ref, tail_ref):
    y = lax.axis_index("y")
    before, running = prefixes(got_ref, y)
    before_ref[...] = before
    tail_ref[...] = tail_before(got_ref, y)
    extras = [got_ref[j, TAIL : TAIL + 16].astype(f32) for j in range(4)]
    line = extras[0] + extras[1] + extras[2] + extras[3]
    extra = jnp.where(iota((16, LANES), 0) == 0, line, extras[3]).astype(bf16)
    for j in range(4):
        pay_ref[j, 0:128] = running
        pay_ref[j, TAIL : TAIL + 16] = extra


def stage_zl(got_ref, before_ref, tail_ref, pay_ref, out_before_ref, out_tail_ref):
    y, zl = lax.axis_index("y"), lax.axis_index("zl")
    before, running = prefixes(got_ref, zl)
    out_before_ref[...] = compose(before, before_ref[...])
    out_tail_ref[...] = jnp.where(y == 0, tail_before(got_ref, zl), tail_ref[...])
    row = iota((16, LANES), 0)
    left = jnp.zeros((16, LANES), f32)
    for j in range(4):
        left = jnp.where(row == j, got_ref[j, TAIL : TAIL + 16].astype(f32)[0:1], left)
    pay_ref[0:128] = running
    pay_ref[TAIL : TAIL + 16] = got_ref[3, TAIL : TAIL + 16]
    pay_ref[LEFT : LEFT + 16] = left.astype(bf16)


def finish(
    got_ref, before_ref, tail_ref, start_ref, ymap_ref, yloc_ref, lines_ref,
    main_ref, pool_ref, matrix_ref, wout_ref, out_ref,
):
    zh, zl, y = lax.axis_index("zh"), lax.axis_index("zl"), lax.axis_index("y")
    state = jnp.concatenate([start_ref[0], start_ref[1]], axis=1)
    pieces = [got_ref[j, :128].astype(f32) for j in range(3)]
    advance = lambda old, piece: mm(old, block_diagonal(piece[:HEAD])) + piece[HEAD:]
    both = compose(pieces[1], pieces[2])
    state = jnp.where(zh > 0, advance(state, pieces[0]), state)
    after = jnp.where(zh > 2, both, pieces[1])
    state = jnp.where(zh > 1, advance(state, after), state)
    state = advance(state, before_ref[...])
    state = state - jnp.mean(state, axis=0, keepdims=True)
    off = yloc_ref[0] + mm(ymap_ref[...], block_diagonal(state), NT)
    row = iota((ROWS, LANES), 0)
    col = iota((ROWS, LANES), 1)
    mean = jnp.where((row // HEAD) == (col // HEAD), 1.0 / HEAD, 0.0).astype(bf16)
    spread = mm_exact_right(off * off, mean)
    headed = off * lax.rsqrt(spread + 1e-05 * HEAD) * lines_ref[4:5] + lines_ref[5:6] + yloc_ref[1]
    attn = (headed * yloc_ref[2]).astype(bf16)

    tail = jnp.where((y == 0) & (zl == 0), tail_before(got_ref, zh), tail_ref[...])
    head = main_ref[0:16, 384:512].astype(f32)
    place = ((zh * 4 + zl) * 4 + y) * ROWS
    opening = pool_rows(
        jnp.concatenate([tail, head], axis=0), head, place, matrix_ref[0], lines_ref[6:7]
    ).astype(bf16)
    pool_out = jnp.concatenate([opening, pool_ref[16:]], axis=0)

    acts = jnp.concatenate([attn, pool_out], axis=1)
    last = pool_out[:, 127:128].astype(f32)
    for zpair in range(8):
        rows = []
        for z in (2 * zpair, 2 * zpair + 1):
            for yy in range(4):
                rows.append(wout_ref[yy, 32 * z : 32 * z + 32])
        made = mm(acts, jnp.concatenate(rows, axis=0), NT)
        for half in range(2):
            z = 2 * zpair + half
            line = got_ref[z // 4, LEFT : LEFT + 16].astype(f32)[z % 4 : z % 4 + 1]
            out_ref[:, 128 * z : 128 * z + 128] = (
                made[:, 128 * half : 128 * half + 128] + last * line
            ).astype(bf16)


def add_parts(part_ref, out_ref):
    total = part_ref[0].astype(f32)
    for j in range(1, 8):
        total = total + part_ref[j].astype(f32)
    out_ref[...] = total.astype(bf16)


def on_device(
    tokens, input_norm_scale, input_norm_bias, query_projection, key_projection,
    value_projection, pooling_input_projection, decay_input_weight, rate_input_weight,
    gate_input_weight, decay_output_weight, rate_output_weight, gate_output_weight,
    decay_bias_base, learning_rate_base, key_prenorm_scale, key_learning_scale,
    self_term_weight, head_norm_scale, head_norm_bias, rate_extra_log, decay_extra_log,
    starting_head_state, pooling_group_matrix, pooling_output_scale, output_attention_rows,
    output_pooling_rows,
):
    line = lambda v: v.reshape(1, -1)
    sent, lines = call(
        prepare_tokens, [shaped((4, 128, 512), bf16), shaped((8, 128), f32)],
        tokens, line(input_norm_scale), line(input_norm_bias), line(decay_bias_base),
        line(learning_rate_base), line(key_prenorm_scale), line(key_learning_scale),
        line(head_norm_scale), line(head_norm_bias), line(pooling_output_scale),
        line(self_term_weight), name="prepare_tokens",
        space=pltpu.HBM, vmem=60 * 2**20,
        scratch=[
            pltpu.VMEM((128, 2048), bf16), pltpu.VMEM((1, 2048), f32), pltpu.VMEM((1, 2048), f32),
            pltpu.SemaphoreType.DMA((11,)),
        ],
    )
    shard, left = call(
        prepare_weights, [shaped((32, 1023), bf16), shaped((16, 128), f32)],
        query_projection, key_projection, value_projection, pooling_input_projection,
        decay_input_weight, rate_input_weight, gate_input_weight, output_attention_rows.T,
        output_pooling_rows.T, name="prepare_weights",
    )
    gathered = lax.all_gather(shard, Z, axis=0, tiled=True)
    mixed_tokens = lax.all_to_all(sent, "y", 0, 0, tiled=True).reshape(512, 512)
    parts, lines, columns = call(
        partial_products,
        [shaped((4, 128, 768), bf16), shaped((8, 128), f32), shaped((512, 256), bf16)],
        mixed_tokens, gathered, lines, name="partial_products",
    )
    parts = lax.all_to_all(parts, "y", 0, 0, tiled=True)
    main, low = call(
        sum_parts, [shaped((128, 512), bf16), shaped((128, 256), bf16)], parts, name="sum_parts"
    )
    low = lax.all_gather(low, "c", axis=0)
    pay, solved, hats, first, wide, columns = call(
        block_maps,
        [
            shaped((4, PAY, 128), bf16), shaped((2, 128, 128), bf16), shaped((3, 128, 128), bf16),
            shaped((128, 128), bf16), shaped((2, 128, 128), f32), shaped((4, 512, 256), bf16),
        ],
        main, low, decay_output_weight, rate_output_weight, lines, rate_extra_log,
        decay_extra_log, left, columns, name="block_maps",
        places=[pl.BlockSpec(memory_space=pltpu.VMEM)] * 5 + [pl.BlockSpec(memory_space=pltpu.HBM)],
        scratch=[pltpu.SemaphoreType.DMA((4,))],
    )
    got = lax.all_to_all(pay, "y", 0, 0, tiled=True)
    pay, before, tail = call(
        stage_y,
        [shaped((4, PAY, 128), bf16), shaped((128, 128), f32), shaped((16, 128), f32)],
        got, name="stage_y",
    )
    got = lax.all_to_all(pay, "zl", 0, 0, tiled=True)
    columns, got, solved = lax.optimization_barrier((columns, got, solved))
    columns = lax.all_to_all(columns, "y", 0, 0, tiled=True)
    y_map, y_local, pool_out = call(
        block_readings,
        [shaped((128, 128), bf16), shaped((3, 128, 128), f32), shaped((128, 128), bf16)],
        main, low, gate_output_weight, solved, hats, first, wide, lines, pooling_group_matrix,
        name="block_readings",
    )
    pay, before, tail = call(
        stage_zl,
        [shaped((WIDE, 128), bf16), shaped((128, 128), f32), shaped((16, 128), f32)],
        got, before, tail, name="stage_zl",
    )
    got = lax.all_gather(pay, "zh", axis=0)
    out = call(
        finish, shaped((128, 2048), bf16),
        got, before, tail, starting_head_state, y_map, y_local, lines, main, pool_out,
        pooling_group_matrix, columns, name="finish",
    )
    parts = lax.all_to_all(out.reshape(8, 16, 2048), TP, 0, 0, tiled=True)
    return call(add_parts, shaped((16, 2048), bf16), parts, name="add_parts")


def solution(mesh):
    split = Mesh(mesh.devices.reshape(4, 4, 4, 4, 2), ("zh", "zl", "y", "x", "c"))
    in_specs = (
        P(SP, None), P(), P(),
        P(SP, TP), P(SP, TP), P(SP, TP), P(SP, TP),
        P(SP, None), P(SP, None), P(SP, None),
        P(None, TP), P(None, TP), P(None, TP),
        P(TP), P(TP), P(TP), P(TP), P(TP), P(TP), P(TP),
        P(SP, TP), P(SP, TP),
        P(TP, None, None), P(TP, None, None), P(TP),
        P(TP, SP), P(TP, SP),
    )
    out_specs = P((*SP, *TP), None)
    return jax.shard_map(
        on_device, mesh=split, in_specs=in_specs, out_specs=out_specs, check_vma=False
    )
```

```python
import functools

import jax
import jax.numpy as jnp
from jax import lax
from jax.experimental import pallas as pl
from jax.experimental.pallas import tpu as pltpu
from jax.sharding import Mesh
from jax.sharding import PartitionSpec as P

Z = ("zh", "zl")
SP = ("zh", "zl", "y")
TP = ("x", "c")
f32 = jnp.float32
bf16 = jnp.bfloat16
HEAD = 64
CHUNK = 64
ROWS = 128
LANES = 128
PAY = 144
WIDE = 160
TAIL = 128
LEFT = 144
NT = (((1,), (1,)), ((), ()))
TN = (((0,), (0,)), ((), ()))


def iota(shape, dim):
    return lax.broadcasted_iota(jnp.int32, shape, dim)


def mm(a, b, dims=(((1,), (0,)), ((), ()))):
    return lax.dot_general(a.astype(bf16), b.astype(bf16), dims, preferred_element_type=f32)


def split(x, parts):
    found = []
    for _ in range(parts):
        piece = x.astype(bf16)
        found.append(piece)
        x = x - piece.astype(f32)
    return found


def mm_exact_right(x, exact):
    return jnp.dot(
        jnp.concatenate(split(x, 3), axis=1),
        jnp.concatenate([exact] * 3, axis=0),
        preferred_element_type=f32,
    )


def mm_exact_left(exact, x):
    return jnp.dot(
        jnp.concatenate([exact] * 3, axis=1),
        jnp.concatenate(split(x, 3), axis=0),
        preferred_element_type=f32,
    )


def mm_wide(a, b):
    a0, a1 = split(a, 2)
    b0, b1 = split(b, 2)
    return jnp.dot(
        jnp.concatenate([a0, a0, a1], axis=1),
        jnp.concatenate([b0, b1, b0], axis=0),
        preferred_element_type=f32,
    )


def call(kernel, outs, *args, flops=10**8, name=None, vmem=16 * 2**20, space=pltpu.VMEM, scratch=()):
    size = sum(a.size * a.dtype.itemsize for a in args)
    return pl.pallas_call(
        kernel,
        out_shape=outs,
        in_specs=[pl.BlockSpec(memory_space=space)] * len(args),
        out_specs=jax.tree.map(lambda _: pl.BlockSpec(memory_space=pltpu.VMEM), outs),
        scratch_shapes=scratch,
        compiler_params=pltpu.CompilerParams(vmem_limit_bytes=vmem),
        cost_estimate=pl.CostEstimate(flops=flops, bytes_accessed=size, transcendentals=0),
        name=name,
    )(*args)


def shaped(shape, dtype):
    return jax.ShapeDtypeStruct(shape, dtype)


def prepare_tokens(tok_hbm, gain_hbm, bias_hbm, *rest):
    *vectors, out_ref, lines_ref, tok, gain, bias, sems = rest
    lines = [
        pltpu.make_async_copy(ref, lines_ref.at[pl.ds(i, 1)], sems.at[3 + i])
        for i, ref in enumerate(vectors)
    ]
    copies = [
        pltpu.make_async_copy(tok_hbm, tok, sems.at[0]),
        pltpu.make_async_copy(gain_hbm, gain, sems.at[1]),
        pltpu.make_async_copy(bias_hbm, bias, sems.at[2]),
        *lines,
    ]
    for copy in copies:
        copy.start()
    source = iota((512, 512), 0)
    target = iota((512, 512), 1)
    moved = ((source >> 5) & 3) * 128 + (source >> 7) * 32 + (source & 31)
    pick = jnp.where(moved == target, 1.0, 0.0).astype(bf16)
    for copy in copies:
        copy.wait()
    wide = tok[...].astype(f32)
    center = jnp.mean(wide, axis=-1, keepdims=True)
    off = wide - center
    spread = jnp.mean(jnp.square(off), axis=-1, keepdims=True)
    normed = (off * lax.rsqrt(spread + 1e-05) * gain[...] + bias[...]).astype(bf16)
    for j in range(4):
        turned = jnp.dot(normed[:, 512 * j : 512 * j + 512], pick, preferred_element_type=f32)
        for y in range(4):
            out_ref[y, :, 128 * j : 128 * j + 128] = turned[:, 128 * y : 128 * y + 128].astype(bf16)


def prepare_weights(
    q_ref, k_ref, v_ref, p_ref, d_ref, r_ref, g_ref, oa_ref, op_ref, out_ref, left_ref
):
    first = lax.axis_index("c") == 0
    out_ref[:, 0:128] = q_ref[...]
    out_ref[:, 128:256] = k_ref[...]
    out_ref[:, 256:384] = v_ref[...]
    out_ref[:, 384:512] = p_ref[...]
    gate = g_ref[...]
    out_ref[:, 512:640] = jnp.where(first, d_ref[...], gate[:, :128])
    out_ref[:, 640:768] = jnp.where(first, r_ref[...], gate[:, 128:])
    out_ref[:, 768:896] = oa_ref[...]
    out_ref[:, 896:1023] = op_ref[:, :127]
    spot = iota((32, LANES), 1) == lax.axis_index("y") * 32 + iota((32, LANES), 0)
    column = op_ref[...].astype(f32)[:, 127:128]
    line = jnp.sum(jnp.where(spot, column, 0.0), axis=0, keepdims=True)
    left_ref[...] = jnp.where(iota((16, LANES), 0) == 0, line, 0.0)


def partial_products(tok_ref, w_ref, lines_ref, part_ref, out_lines_ref):
    out_lines_ref[...] = lines_ref[...]
    made = jnp.dot(tok_ref[...], w_ref[:, :768], preferred_element_type=f32).astype(bf16)
    for y in range(4):
        part_ref[y] = made[128 * y : 128 * y + 128]


def spread_columns(w_ref, out_ref):
    first = w_ref[:, 768:896]
    second = w_ref[:, 896:1023]
    for y in range(4):
        out_ref[y, :, 0:128] = first
        out_ref[y, :, 128:255] = second
        out_ref[y, :, 255:256] = jnp.zeros((512, 1), bf16)


def sum_parts(part_ref, main_ref, low_ref):
    total = part_ref[0].astype(f32)
    for y in range(1, 4):
        total = total + part_ref[y].astype(f32)
    rounded = total.astype(bf16)
    main_ref[...] = rounded[:, :512]
    low = rounded[:, 512:].astype(f32)
    first = lax.axis_index("c") == 0
    one = jnp.where(first, jnp.tanh(low[:, :128]), jax.nn.sigmoid(low[:, :128]))
    two = jnp.where(first, low[:, 128:], jax.nn.sigmoid(low[:, 128:]))
    low_ref[:, :128] = one.astype(bf16)
    low_ref[:, 128:] = two.astype(bf16)


def masked(x, lane_low):
    zero = jnp.zeros_like(x)
    return [jnp.where(lane_low, x, zero), jnp.where(lane_low, zero, x)]


def block_diagonal(pair):
    low = iota(pair.shape, 1) < HEAD
    zero = jnp.zeros_like(pair)
    return jnp.concatenate([jnp.where(low, pair, zero), jnp.where(low, zero, pair)], axis=0)


def block_maps(
    main_ref, low_ref, dw_ref, rw_ref, lines_ref, re_ref, de_ref, left_ref, pay_ref, solved_ref, hats_ref, first_ref, wide_ref,
):
    line = lambda i: lines_ref[i : i + 1]
    recept = main_ref[:, 0:128].astype(f32)
    keys = main_ref[:, 128:256].astype(f32)
    values_b = main_ref[:, 256:384]
    row = iota((ROWS, LANES), 0)
    col = iota((ROWS, LANES), 1)
    lane_low = col < HEAD
    same = (row // CHUNK) == (col // CHUNK)

    drive = line(0) + jnp.dot(low_ref[0, :, :128], dw_ref[...], preferred_element_type=f32)
    log_decay = -jax.nn.sigmoid(drive) * jnp.exp(re_ref[...] - 0.5) + de_ref[...]
    rate = jax.nn.sigmoid(
        line(1) + jnp.dot(low_ref[0, :, 128:], rw_ref[...], preferred_element_type=f32)
    )

    ones = jnp.where(same, 1.0, 0.0).astype(bf16)
    unit = keys * line(2)
    effective = keys * (1.0 + (rate - 1.0) * line(3))
    unit = unit * lax.rsqrt(mm_exact_right(unit * unit, ones) + 1e-06)
    wide_ref[1] = recept * effective
    beta = unit * rate

    tril = jnp.where(same & (row >= col), 1.0, 0.0).astype(bf16)
    totals = mm_exact_left(jnp.concatenate([tril, ones], axis=0), log_decay)
    total, end = totals[:ROWS], totals[ROWS:]
    ref = 0.5 * end
    grow = jnp.exp(ref - total)
    shrink = jnp.exp(total - ref)
    base = jnp.exp(ref)
    a_hat = -unit * jnp.exp(total - log_decay - ref)
    r_hat = recept * shrink
    b_hat = beta * grow
    k_hat = effective * grow
    wide_ref[0] = r_hat * base
    hats_ref[0] = r_hat.astype(bf16)
    hats_ref[1] = b_hat.astype(bf16)
    hats_ref[2] = k_hat.astype(bf16)

    left = jnp.concatenate(masked(a_hat, lane_low), axis=0)
    right = jnp.concatenate([b_hat, k_hat], axis=0)
    scores = mm(left, right, NT)
    strict = same & (row > col)
    eye = jnp.where(row == col, 1.0, 0.0).astype(f32)
    swapped = pltpu.roll(a_hat * base, HEAD, 1)
    full = [jnp.where(strict, scores[h * ROWS : h * ROWS + ROWS, :ROWS], 0.0) for h in range(2)]
    within = {n: (row // n) == (col // n) for n in (8, 16, 32)}
    power = [jnp.where(within[8], full[h], 0.0) for h in range(2)]
    product = [eye + power[h] for h in range(2)]
    for _ in range(2):
        power = [mm_wide(power[h], power[h]) for h in range(2)]
        product = [product[h] + mm_wide(product[h], power[h]) for h in range(2)]
    for here in (within[16] & ~within[8], within[32] & ~within[16]):
        mid = [mm_wide(product[h], jnp.where(here, full[h], 0.0)) for h in range(2)]
        product = [product[h] + mm_wide(mid[h], product[h]) for h in range(2)]
    solved = []
    for h in range(2):
        pushed = mm(jnp.where(strict, scores[h * ROWS : h * ROWS + ROWS, ROWS:], 0.0), values_b)
        rhs = jnp.where(lane_low if h == 0 else ~lane_low, pushed, swapped)
        part = mm(product[h], rhs)
        across = jnp.where(within[32], 0.0, full[h])
        solved.append((part + mm(product[h], mm(across, part))).astype(bf16))
        solved_ref[h] = solved[h]

    b_end = (b_hat * base).astype(bf16)
    k_end = (k_hat * base).astype(bf16)
    decay_end = jnp.exp(end)
    low64 = iota((CHUNK, LANES), 1) < HEAD
    diagonal = iota((CHUNK, LANES), 0) == (iota((CHUNK, LANES), 1) % HEAD)
    maps, states = [], []
    for c in range(2):
        at = slice(c * CHUNK, c * CHUNK + CHUNK)
        g0 = mm(solved[0][at], b_end[at], TN)
        g1 = mm(solved[1][at], b_end[at], TN)
        kv = mm(values_b[at], k_end[at], TN)
        maps.append(
            jnp.where(diagonal, decay_end[at], 0.0) + jnp.where(low64, g0[HEAD:], g1[:HEAD])
        )
        states.append(
            jnp.where(low64, g0[:HEAD], g1[HEAD:]) + jnp.where(low64, kv[:HEAD], kv[HEAD:])
        )
    chunk0 = jnp.concatenate([maps[0], states[0]], axis=0).astype(bf16)
    first_ref[...] = chunk0
    joined = mm(chunk0, block_diagonal(maps[1]))
    block_map = joined[:CHUNK].astype(bf16)
    block_state = (joined[CHUNK:] + states[1]).astype(bf16)
    tail = main_ref[ROWS - 16 :, 384:512].astype(f32)
    extra = jnp.where(row[:16] == 0, left_ref[...], tail).astype(bf16)
    for j in range(4):
        pay_ref[j, 0:64] = block_map
        pay_ref[j, 64:128] = block_state
        pay_ref[j, TAIL : TAIL + 16] = extra


def pool_rows(extended, own, place, matrix, scale):
    level = lax.axis_index("x")
    sums = extended
    chosen = None
    for k in range(4):
        width = 1 << k
        sums = sums + pltpu.roll(sums, width, 0)
        picked = sums[16:]
        chosen = picked if k == 0 else jnp.where(level >= k, picked, chosen)
    window = lax.shift_left(jnp.int32(2), level).astype(f32)
    position = (place + iota(own.shape, 0)).astype(f32)
    pooled = (chosen / jnp.minimum(position + 1.0, window) - own).astype(bf16)
    return jnp.dot(pooled, matrix, preferred_element_type=f32) * scale


def block_readings(
    main_ref, low_ref, gw_ref, solved_ref, hats_ref, first_ref, wide_ref, lines_ref, matrix_ref,
    ymap_ref, out_ref, pool_ref,
):
    pool = main_ref[:, 384:512].astype(f32)
    place = ((lax.axis_index("zh") * 4 + lax.axis_index("zl")) * 4 + lax.axis_index("y")) * ROWS
    pool_ref[0:16] = jnp.zeros((16, LANES), bf16)
    pool_ref[16:] = pool_rows(
        pool, pool[16:], place + 16, matrix_ref[0], lines_ref[6:7]
    ).astype(bf16)
    values_b = main_ref[:, 256:384]
    row = iota((ROWS, LANES), 0)
    col = iota((ROWS, LANES), 1)
    lane_low = col < HEAD
    upto = ((row // CHUNK) == (col // CHUNK)) & (row >= col)
    heads = (row // HEAD) == (col // HEAD)
    ones = jnp.where(heads, 1.0, 0.0).astype(bf16)
    out_ref[1] = mm_exact_right(wide_ref[1] * lines_ref[7:8], ones) * values_b.astype(f32)
    out_ref[2] = jnp.dot(low_ref[1], gw_ref[...], preferred_element_type=f32)
    scores = mm(
        jnp.concatenate(masked(hats_ref[0].astype(f32), lane_low), axis=0),
        jnp.concatenate([hats_ref[1], hats_ref[2]], axis=0),
        NT,
    )
    reads, direct = [], []
    for h in range(2):
        at = slice(h * ROWS, h * ROWS + ROWS)
        reads.append(mm(jnp.where(upto, scores[at, :ROWS], 0.0), solved_ref[h]))
        direct.append(mm(jnp.where(upto, scores[at, ROWS:], 0.0), values_b))
    y_local = jnp.where(lane_low, reads[0] + direct[0], reads[1] + direct[1])
    y_map = wide_ref[0] + pltpu.roll(jnp.where(lane_low, reads[1], reads[0]), HEAD, 1)
    first = first_ref[...].astype(f32)
    late = mm(
        y_map[CHUNK:],
        jnp.concatenate([block_diagonal(first[CHUNK:]), block_diagonal(first[:CHUNK])], axis=0),
        NT,
    )
    ymap_ref[:CHUNK] = y_map[:CHUNK].astype(bf16)
    ymap_ref[CHUNK:] = late[:, LANES:].astype(bf16)
    y_local = jnp.concatenate([y_local[:CHUNK], y_local[CHUNK:] + late[:, :LANES]], axis=0)
    mean = jnp.where(heads, 1.0 / HEAD, 0.0).astype(bf16)
    out_ref[0] = y_local - mm_exact_right(y_local, mean)


def identity_pair():
    eye = iota((HEAD, LANES), 0) == (iota((HEAD, LANES), 1) % HEAD)
    return jnp.concatenate([jnp.where(eye, 1.0, 0.0).astype(f32), jnp.zeros((HEAD, LANES), f32)], 0)


def compose(earlier, later):
    moved = mm(earlier, block_diagonal(later[:HEAD]))
    return jnp.concatenate([moved[:HEAD], moved[HEAD:] + later[HEAD:]], axis=0)


def tail_before(got_ref, mine):
    found = jnp.zeros((16, LANES), f32)
    for j in range(3):
        found = jnp.where(mine == j + 1, got_ref[j, TAIL : TAIL + 16].astype(f32), found)
    return found


def prefixes(got_ref, mine):
    pieces = [got_ref[j, :128].astype(f32) for j in range(4)]
    two = compose(pieces[0], pieces[1])
    three = compose(two, pieces[2])
    whole = compose(two, compose(pieces[2], pieces[3]))
    before = jnp.where(mine == 0, identity_pair(), pieces[0])
    before = jnp.where(mine > 1, two, before)
    before = jnp.where(mine > 2, three, before)
    return before, whole.astype(bf16)


def stage_y(got_ref, pay_ref, before_ref, tail_ref):
    y = lax.axis_index("y")
    before, running = prefixes(got_ref, y)
    before_ref[...] = before
    tail_ref[...] = tail_before(got_ref, y)
    extras = [got_ref[j, TAIL : TAIL + 16].astype(f32) for j in range(4)]
    line = extras[0] + extras[1] + extras[2] + extras[3]
    extra = jnp.where(iota((16, LANES), 0) == 0, line, extras[3]).astype(bf16)
    for j in range(4):
        pay_ref[j, 0:128] = running
        pay_ref[j, TAIL : TAIL + 16] = extra


def stage_zl(got_ref, before_ref, tail_ref, pay_ref, out_before_ref, out_tail_ref):
    y, zl = lax.axis_index("y"), lax.axis_index("zl")
    before, running = prefixes(got_ref, zl)
    out_before_ref[...] = compose(before, before_ref[...])
    out_tail_ref[...] = jnp.where(y == 0, tail_before(got_ref, zl), tail_ref[...])
    row = iota((16, LANES), 0)
    left = jnp.zeros((16, LANES), f32)
    for j in range(4):
        left = jnp.where(row == j, got_ref[j, TAIL : TAIL + 16].astype(f32)[0:1], left)
    pay_ref[0:128] = running
    pay_ref[TAIL : TAIL + 16] = got_ref[3, TAIL : TAIL + 16]
    pay_ref[LEFT : LEFT + 16] = left.astype(bf16)


def finish(
    got_ref, before_ref, tail_ref, start_ref, ymap_ref, yloc_ref, lines_ref,
    main_ref, pool_ref, matrix_ref, wout_ref, out_ref,
):
    zh, zl, y = lax.axis_index("zh"), lax.axis_index("zl"), lax.axis_index("y")
    state = jnp.concatenate([start_ref[0], start_ref[1]], axis=1)
    pieces = [got_ref[j, :128].astype(f32) for j in range(3)]
    advance = lambda old, piece: mm(old, block_diagonal(piece[:HEAD])) + piece[HEAD:]
    both = compose(pieces[1], pieces[2])
    state = jnp.where(zh > 0, advance(state, pieces[0]), state)
    after = jnp.where(zh > 2, both, pieces[1])
    state = jnp.where(zh > 1, advance(state, after), state)
    state = advance(state, before_ref[...])
    state = state - jnp.mean(state, axis=0, keepdims=True)
    off = yloc_ref[0] + mm(ymap_ref[...], block_diagonal(state), NT)
    row = iota((ROWS, LANES), 0)
    col = iota((ROWS, LANES), 1)
    mean = jnp.where((row // HEAD) == (col // HEAD), 1.0 / HEAD, 0.0).astype(bf16)
    spread = mm_exact_right(off * off, mean)
    headed = off * lax.rsqrt(spread + 1e-05 * HEAD) * lines_ref[4:5] + lines_ref[5:6] + yloc_ref[1]
    attn = (headed * yloc_ref[2]).astype(bf16)

    tail = jnp.where((y == 0) & (zl == 0), tail_before(got_ref, zh), tail_ref[...])
    head = main_ref[0:16, 384:512].astype(f32)
    place = ((zh * 4 + zl) * 4 + y) * ROWS
    opening = pool_rows(
        jnp.concatenate([tail, head], axis=0), head, place, matrix_ref[0], lines_ref[6:7]
    ).astype(bf16)
    pool_out = jnp.concatenate([opening, pool_ref[16:]], axis=0)

    acts = jnp.concatenate([attn, pool_out], axis=1)
    last = pool_out[:, 127:128].astype(f32)
    for zpair in range(8):
        rows = []
        for z in (2 * zpair, 2 * zpair + 1):
            for yy in range(4):
                rows.append(wout_ref[yy, 32 * z : 32 * z + 32])
        made = mm(acts, jnp.concatenate(rows, axis=0), NT)
        for half in range(2):
            z = 2 * zpair + half
            line = got_ref[z // 4, LEFT : LEFT + 16].astype(f32)[z % 4 : z % 4 + 1]
            out_ref[:, 128 * z : 128 * z + 128] = (
                made[:, 128 * half : 128 * half + 128] + last * line
            ).astype(bf16)


def add_parts(part_ref, out_ref):
    total = part_ref[0].astype(f32)
    for j in range(1, 8):
        total = total + part_ref[j].astype(f32)
    out_ref[...] = total.astype(bf16)


def on_device(
    tokens, input_norm_scale, input_norm_bias, query_projection, key_projection,
    value_projection, pooling_input_projection, decay_input_weight, rate_input_weight,
    gate_input_weight, decay_output_weight, rate_output_weight, gate_output_weight,
    decay_bias_base, learning_rate_base, key_prenorm_scale, key_learning_scale,
    self_term_weight, head_norm_scale, head_norm_bias, rate_extra_log, decay_extra_log,
    starting_head_state, pooling_group_matrix, pooling_output_scale, output_attention_rows,
    output_pooling_rows,
):
    line = lambda v: v.reshape(1, -1)
    sent, lines = call(
        prepare_tokens, [shaped((4, 128, 512), bf16), shaped((8, 128), f32)],
        tokens, line(input_norm_scale), line(input_norm_bias), line(decay_bias_base),
        line(learning_rate_base), line(key_prenorm_scale), line(key_learning_scale),
        line(head_norm_scale), line(head_norm_bias), line(pooling_output_scale),
        line(self_term_weight), name="prepare_tokens",
        space=pltpu.HBM, vmem=60 * 2**20,
        scratch=[
            pltpu.VMEM((128, 2048), bf16), pltpu.VMEM((1, 2048), f32), pltpu.VMEM((1, 2048), f32),
            pltpu.SemaphoreType.DMA((11,)),
        ],
    )
    shard, left = call(
        prepare_weights, [shaped((32, 1023), bf16), shaped((16, 128), f32)],
        query_projection, key_projection, value_projection, pooling_input_projection,
        decay_input_weight, rate_input_weight, gate_input_weight, output_attention_rows.T,
        output_pooling_rows.T, name="prepare_weights",
    )
    gathered = lax.all_gather(shard, Z, axis=0, tiled=True)
    mixed_tokens = lax.all_to_all(sent, "y", 0, 0, tiled=True).reshape(512, 512)
    parts, lines = call(
        partial_products, [shaped((4, 128, 768), bf16), shaped((8, 128), f32)],
        mixed_tokens, gathered, lines, name="partial_products",
    )
    parts = lax.all_to_all(parts, "y", 0, 0, tiled=True)
    main, low = call(
        sum_parts, [shaped((128, 512), bf16), shaped((128, 256), bf16)], parts, name="sum_parts"
    )
    low = lax.all_gather(low, "c", axis=0)
    pay, solved, hats, first, wide = call(
        block_maps,
        [
            shaped((4, PAY, 128), bf16), shaped((2, 128, 128), bf16), shaped((3, 128, 128), bf16),
            shaped((128, 128), bf16), shaped((2, 128, 128), f32),
        ],
        main, low, decay_output_weight, rate_output_weight, lines, rate_extra_log,
        decay_extra_log, left, name="block_maps",
    )
    columns, pay = lax.optimization_barrier((gathered, pay))
    got = lax.all_to_all(pay, "y", 0, 0, tiled=True)
    columns = call(spread_columns, shaped((4, 512, 256), bf16), columns, name="spread_columns")
    y_map, y_local, pool_out = call(
        block_readings,
        [shaped((128, 128), bf16), shaped((3, 128, 128), f32), shaped((128, 128), bf16)],
        main, low, gate_output_weight, solved, hats, first, wide, lines, pooling_group_matrix,
        name="block_readings",
    )
    pay, before, tail = call(
        stage_y,
        [shaped((4, PAY, 128), bf16), shaped((128, 128), f32), shaped((16, 128), f32)],
        got, name="stage_y",
    )
    got = lax.all_to_all(pay, "zl", 0, 0, tiled=True)
    columns, got, y_map = lax.optimization_barrier((columns, got, y_map))
    columns = lax.all_to_all(columns, "y", 0, 0, tiled=True)
    pay, before, tail = call(
        stage_zl,
        [shaped((WIDE, 128), bf16), shaped((128, 128), f32), shaped((16, 128), f32)],
        got, before, tail, name="stage_zl",
    )
    got = lax.all_gather(pay, "zh", axis=0)
    out = call(
        finish, shaped((128, 2048), bf16),
        got, before, tail, starting_head_state, y_map, y_local, lines, main, pool_out,
        pooling_group_matrix, columns, name="finish",
    )
    parts = lax.all_to_all(out.reshape(8, 16, 2048), TP, 0, 0, tiled=True)
    return call(add_parts, shaped((16, 2048), bf16), parts, name="add_parts")


def solution(mesh):
    split = Mesh(mesh.devices.reshape(4, 4, 4, 4, 2), ("zh", "zl", "y", "x", "c"))
    in_specs = (
        P(SP, None), P(), P(),
        P(SP, TP), P(SP, TP), P(SP, TP), P(SP, TP),
        P(SP, None), P(SP, None), P(SP, None),
        P(None, TP), P(None, TP), P(None, TP),
        P(TP), P(TP), P(TP), P(TP), P(TP), P(TP), P(TP),
        P(SP, TP), P(SP, TP),
        P(TP, None, None), P(TP, None, None), P(TP),
        P(TP, SP), P(TP, SP),
    )
    out_specs = P((*SP, *TP), None)
    return jax.shard_map(
        on_device, mesh=split, in_specs=in_specs, out_specs=out_specs, check_vma=False
    )
```
